256 devices in a mesh: ep: 64 (over z, x, core), tp: 4 (over y).
Axes of the slice: x: 4, y: 4, z: 8, core: 2. Of those that a mesh axis runs over, the one named last changes fastest.
Arguments:
- queries: bfloat16 [8192, 2048], P('ep', 'tp'), may hold values from -60 to 60
- keys: bfloat16 [8192, 512], P('ep', 'tp'), may hold values from -60 to 60
- values: bfloat16 [8192, 512], P('ep', 'tp'), may hold values from -6 to 6
- cum_gates: float32 [8192, 16], P('ep', 'tp'), may hold values from -2051 to 0, as said below
- expert_in: bfloat16 [32768, 4096], P(('ep', 'tp')), may hold values from -6 to 6
- norm_gain: float32 [4096], replicated, may hold values from 0.1 to 1.9
- route_group: int32 [32768, 1], P(('ep', 'tp')), may hold values from 0 to 63; in each aligned block of 128 rows (0 to 127, 128 to 255, ...) at most 3 rows name the same one
- route_member: int32 [32768, 2], P(('ep', 'tp')), may hold values from 0 to 3, all different within a row
- route_weight: float32 [32768, 2], P(('ep', 'tp')), may hold values from 0.1 to 1
- w_gate: bfloat16 [256, 4096, 384], P(('ep', 'tp')), may hold values from -0.09375 to 0.09375
- w_up: bfloat16 [256, 4096, 384], P(('ep', 'tp')), may hold values from -0.09375 to 0.09375
- w_down: bfloat16 [256, 384, 4096], P(('ep', 'tp')), may hold values from -0.3125 to 0.3125
Outputs:
- attended: bfloat16 [8192, 2048], P('ep', 'tp')
- expert_out: bfloat16 [32768, 4096], P(('ep', 'tp'))
The draws below stay inside these ranges and needn't reach their ends.
Inputs may be any that keep to these rules, and one draw needn't show every extreme that they name: `cum_gates`: each head's entries never rise along positions. `route_group`: at most 3 of the rows of one device name one group. `route_member`: the 2 entries of a row differ.
All inputs are finite; a program needn't handle non-finite values.
Results may differ from the reference program's by a relative error of at most 0.0075.
Values may be sent and summed in bfloat16 or wider, within the bound.
A program may use at most 128 MiB of HBM per device.

```python
import math
import jax
import jax.numpy as jnp
import numpy as np
from jax import lax

D = 4096
HEAD_WIDTH = 128
QUERY_HEADS = 16
KEY_VALUE_HEADS = 4
FF = 384
GROUP = 4
TOP = 2
TOK_A = 128
TOK_B = 128
ATTENDED_LENGTH = 8192
TOKENS_B = 32768
CAP = 3
EXPERTS = 256
N_EP = 64
N_TP = 4


def draw_keys(key, part):
    base_value = jax.random.normal(jax.random.fold_in(key, 1), (ATTENDED_LENGTH, KEY_VALUE_HEADS, HEAD_WIDTH), jnp.float32)
    return base_value.reshape(ATTENDED_LENGTH, KEY_VALUE_HEADS * HEAD_WIDTH).astype(jnp.bfloat16)


def draw_queries(key, part):
    heads_per_group = QUERY_HEADS // KEY_VALUE_HEADS
    base_value = jax.random.normal(jax.random.fold_in(key, 2), (ATTENDED_LENGTH, KEY_VALUE_HEADS, heads_per_group, HEAD_WIDTH), jnp.float32)
    return base_value.reshape(ATTENDED_LENGTH, QUERY_HEADS * HEAD_WIDTH).astype(jnp.bfloat16)


def draw_cum_gates(key, part):
    share = 0.5
    slow_heads = jax.random.uniform(jax.random.fold_in(key, 3), (QUERY_HEADS,), jnp.float32) < share
    slow_rate = jnp.exp(jax.random.uniform(jax.random.fold_in(key, 4), (QUERY_HEADS,), jnp.float32, math.log(0.3), 0.0)) / ATTENDED_LENGTH
    fast_rate = 1.0 / jnp.exp(jax.random.uniform(jax.random.fold_in(key, 5), (QUERY_HEADS,), jnp.float32, math.log(30.0), math.log(100.0)))
    rates = jnp.where(slow_heads, slow_rate, fast_rate)
    block_count = ATTENDED_LENGTH // TOK_A
    block_factor = jnp.exp(jax.random.uniform(jax.random.fold_in(key, 6), (block_count,), jnp.float32, math.log(0.5), math.log(2.0)))
    position_factor = jnp.repeat(block_factor, TOK_A)
    roughness = jax.random.uniform(jax.random.fold_in(key, 7), (ATTENDED_LENGTH, QUERY_HEADS), jnp.float32, 0.2, 1.8)
    gate_logarithms = -rates[None, :] * position_factor[:, None] * roughness
    spike_positions = jax.random.randint(jax.random.fold_in(key, 8), (3,), 1, ATTENDED_LENGTH)
    spike_loss = jax.random.uniform(jax.random.fold_in(key, 9), (3, QUERY_HEADS), jnp.float32, 0.2, 0.5)
    spike_values = jnp.zeros((ATTENDED_LENGTH, QUERY_HEADS), jnp.float32).at[spike_positions].add(jnp.log1p(-spike_loss))
    return jnp.cumsum(gate_logarithms + spike_values, axis=0)


def shard_levels(stream_key, dims, pieces, least, largest):
    factor_of, own = 1.0, jax.random.fold_in(stream_key, 6)
    for dim, shards_of in pieces:
        draws = jnp.exp(jax.random.uniform(jax.random.fold_in(own, dim), (shards_of,), jnp.float32, least / len(pieces), largest / len(pieces)))
        factor_of = factor_of * jnp.repeat(draws, dims[dim] // shards_of).reshape([-1 if axis == dim else 1 for axis in range(len(dims))])
    return factor_of


def choose_distinct(key, rows, count, top, lift):
    order = jax.random.permutation(jax.random.fold_in(key, 1), count)
    boost = order
    for power in range(3):
        boost = boost * boost // count
    boost = boost * lift // count
    chance = jax.random.randint(jax.random.fold_in(key, 2), (rows, count), 0, 4096) + boost
    sure = jax.random.permutation(jax.random.fold_in(key, 3), rows)[jnp.arange(count) % rows]
    chance = jnp.where(jnp.arange(rows)[:, None] == sure[None, :], 1 << 14, chance)
    priority = chance * count + jnp.arange(count)
    return lax.top_k(priority.astype(jnp.int32), top)[1].astype(jnp.int32)


def routed_block(own_key, own, number, rows, number_of, top, most, slope):
    sequence = jax.random.permutation(own_key, number_of)
    packed, ordinary = portions_of(number_of, rows * top, most, slope, True), portions_of(number_of, rows * top, most, slope, False)
    places = jnp.arange(number_of)

    def named(sizes, turn):
        used = int((sizes > 0).sum())
        fixed = max(1, used // 4)
        moved = fixed + (places - fixed + turn * (used - fixed)) % max(1, number_of - fixed)
        return jnp.zeros((number_of,), jnp.int32).at[sequence[jnp.where(places < fixed, places, moved)]].set(jnp.asarray(sizes, jnp.int32))

    sizes = jnp.where(number % 4 == 0, named(packed, number // 4), named(ordinary, number - number // 4 - 1))
    mixed = jax.random.permutation(jax.random.fold_in(own, 3), number_of)
    source_of, taker = mixed[0:number_of // 2 * 2:2], mixed[1:number_of // 2 * 2:2]
    margin = jnp.minimum(sizes[source_of] - 1, most - sizes[taker]) // 2
    margin = jnp.where((source_of == sequence[0]) | (taker == sequence[0]) | (sizes[taker] == 0), 0, jnp.maximum(margin, 0))
    moved = jax.random.randint(jax.random.fold_in(own, 4), (number_of // 2,), 0, 1 << 20) % (margin + 1)
    sizes = sizes.at[source_of].add(-moved).at[taker].add(moved)
    items = jnp.searchsorted(jnp.cumsum(sizes), jnp.arange(rows * top), side="right").astype(jnp.int32)
    grid = items.reshape(top, rows).T
    grid = grid[jax.random.permutation(jax.random.fold_in(own, 1), rows)]
    turn = jax.random.randint(jax.random.fold_in(own, 2), (rows, 1), 0, top)
    return jnp.take_along_axis(grid, (jnp.arange(top)[None, :] + turn) % top, axis=1)


def portions_of(count, total, reach, slope, full):
    portions = [(1 << 20) // math.isqrt(rank ** slope) + 1 for rank in range(1, count + 1)]
    largest = reach if full else min(reach, max(-(-total // count), total * portions[0] // sum(portions)))
    least = 1 if total - largest >= count - 1 else 0
    holding, spare = [largest] + [least] * (count - 1), total - largest - least * (count - 1)
    while spare > 0:
        candidates = [i for i in range(1, count) if holding[i] < largest] or [i for i in range(1, count) if holding[i] < reach]
        pool, left = sum([portions[i] for i in candidates]), spare
        for i in candidates:
            extra = min(reach - holding[i], max(1, left * portions[i] // pool), spare)
            holding[i] = holding[i] + extra
            spare = spare - extra
    return np.array(holding)


def scatter_about(own_key, shape, scale, bound, cuts=(), held_as=jnp.bfloat16):
    level = shard_levels(own_key, shape, cuts, -0.22, 0.18) if cuts else 1.0
    drawn = jax.random.normal(own_key, shape, jnp.float32) * scale * level
    return jnp.minimum(jnp.maximum(drawn, -bound), bound).astype(held_as)


def setup_inputs(seed: int = 0) -> dict:
    seeds = jax.random.split(jax.random.key(seed), 13)
    queries = draw_queries(jax.random.fold_in(seeds[12], 71), 0)
    keys = draw_keys(jax.random.fold_in(seeds[12], 71), 0)
    values = scatter_about(seeds[2], (ATTENDED_LENGTH, KEY_VALUE_HEADS * HEAD_WIDTH), 1.0, 6.0, ((0, 64), (1, 4)))
    cum_gates = draw_cum_gates(jax.random.fold_in(seeds[12], 71), 0)
    expert_in = scatter_about(seeds[4], (TOKENS_B, D), 1.0, 6.0, ((0, 256),))
    norm_gain = jnp.clip(1.0 + 0.18 * jax.random.normal(seeds[5], (D,), jnp.float32), 0.1, 1.9)
    route_group_keys = jax.random.split(jax.random.fold_in(seeds[6], 1), TOKENS_B // TOK_B)
    route_group_turns = jax.random.permutation(jax.random.fold_in(seeds[6], 3), TOKENS_B // TOK_B)
    route_group = jax.vmap(lambda own, number: routed_block(jax.random.fold_in(seeds[6], 2), own, number, TOK_B, N_EP, 1, CAP, 2))(route_group_keys, route_group_turns).reshape((TOKENS_B, 1))
    route_member = choose_distinct(seeds[7], TOKENS_B, GROUP, TOP, 0)
    route_weight = jnp.clip(jnp.exp(math.log(1.0) - 2.3025851 * jax.random.uniform(seeds[8], (TOKENS_B, TOP), jnp.float32) ** shard_levels(seeds[8], (TOKENS_B, TOP), ((0, 256),), -0.2, 0.2)), 0.1, 1.0)
    w_gate = scatter_about(seeds[9], (EXPERTS, D, FF), D ** -0.5, 0.09375, ((0, 256),))
    w_up = scatter_about(seeds[10], (EXPERTS, D, FF), D ** -0.5, 0.09375, ((0, 256),))
    w_down = scatter_about(seeds[11], (EXPERTS, FF, D), FF ** -0.5, 0.3125, ((0, 256),))
    return {"queries": queries, "keys": keys, "values": values, "cum_gates": cum_gates, "expert_in": expert_in, "norm_gain": norm_gain, "route_group": route_group, "route_member": route_member, "route_weight": route_weight, "w_gate": w_gate, "w_up": w_up, "w_down": w_down}


NEGATIVE = -1e+30
EPSILON = 1e-06

def attention_part(queries, keys, values, cum_gates):
    sequence_length = queries.shape[0]
    heads_per_group = QUERY_HEADS // KEY_VALUE_HEADS
    rows_per_block = math.gcd(sequence_length, 512)
    score_scale = HEAD_WIDTH ** (-0.5)
    every_query = queries.reshape(sequence_length, KEY_VALUE_HEADS, heads_per_group, HEAD_WIDTH).astype(jnp.float32)
    every_key = keys.reshape(sequence_length, KEY_VALUE_HEADS, HEAD_WIDTH).astype(jnp.float32)
    every_value = values.reshape(sequence_length, KEY_VALUE_HEADS, HEAD_WIDTH).astype(jnp.float32)

    def query_block(block_index):
        start_row = block_index * rows_per_block
        query_rows = lax.dynamic_slice_in_dim(every_query, start_row, rows_per_block, 0)
        query_gates = lax.dynamic_slice_in_dim(cum_gates, start_row, rows_per_block, 0)
        query_pos = start_row + jnp.arange(rows_per_block, dtype=jnp.int32)

        def key_step(key_index, carried):
            running, totals, accumulated = carried
            key_start = (key_index * rows_per_block).astype(jnp.int32)
            key_rows = lax.dynamic_slice_in_dim(every_key, key_start, rows_per_block, 0)
            rows_of_value = lax.dynamic_slice_in_dim(every_value, key_start, rows_per_block, 0)
            key_gates = lax.dynamic_slice_in_dim(cum_gates, key_start, rows_per_block, 0)
            key_pos = key_start + jnp.arange(rows_per_block, dtype=jnp.int32)
            scores = jnp.einsum('qgrd,kgd->grqk', query_rows, key_rows).reshape(QUERY_HEADS, rows_per_block, rows_per_block) * score_scale
            scores = scores + query_gates.T[:, :, None] - key_gates.T[:, None, :]
            allowed = (key_pos[None, :] <= query_pos[:, None])[None]
            scores = jnp.where(allowed, scores, NEGATIVE)
            new_max = jnp.maximum(running, lax.optimization_barrier(jnp.max(scores, axis=-1)))
            weights = jnp.where(allowed, jnp.exp(scores - new_max[..., None]), 0.0)
            factor = jnp.exp(running - new_max)
            totals = totals * factor + lax.optimization_barrier(jnp.sum(weights, axis=-1))
            rounded_count = lax.optimization_barrier(weights.astype(jnp.bfloat16)).astype(jnp.float32)
            inner_product = jnp.einsum('tjub,btl->tjul', rounded_count.reshape(KEY_VALUE_HEADS, heads_per_group, rows_per_block, rows_per_block), rows_of_value)
            accumulated = accumulated * factor[..., None] + inner_product.reshape(QUERY_HEADS, rows_per_block, HEAD_WIDTH)
            return (new_max, totals, accumulated)
        initial = (jnp.full((QUERY_HEADS, rows_per_block), NEGATIVE, jnp.float32), jnp.zeros((QUERY_HEADS, rows_per_block), jnp.float32), jnp.zeros((QUERY_HEADS, rows_per_block, HEAD_WIDTH), jnp.float32))
        running, totals, accumulated = lax.fori_loop(0, block_index + 1, key_step, initial)
        result = accumulated / totals[..., None]
        return jnp.transpose(result, (1, 0, 2)).reshape(rows_per_block, QUERY_HEADS * HEAD_WIDTH).astype(jnp.bfloat16)
    blocks = lax.map(query_block, jnp.arange(sequence_length // rows_per_block, dtype=jnp.int32))
    return blocks.reshape(sequence_length, QUERY_HEADS * HEAD_WIDTH)

def expert_part(expert_in, norm_gain, route_group, route_member, route_weight, w_gate, w_up, w_down):
    count_rows, model_width = expert_in.shape
    floats = expert_in.astype(jnp.float32)
    normed = (floats * lax.rsqrt(lax.optimization_barrier(jnp.mean(floats * floats, axis=-1, keepdims=True)) + EPSILON) * norm_gain).astype(jnp.bfloat16)
    members = jnp.arange(GROUP, dtype=jnp.int32)
    mix_weights = jnp.zeros((count_rows, GROUP), jnp.float32)
    for rank_index in range(TOP):
        mix_weights = mix_weights + route_weight[:, rank_index:rank_index + 1] * (route_member[:, rank_index:rank_index + 1] == members[None, :]).astype(jnp.float32)
    mix_weights = lax.optimization_barrier(mix_weights.astype(jnp.bfloat16)).astype(jnp.float32)
    group_ids = route_group[:, 0]
    group_match = (group_ids[:, None] == jnp.arange(N_EP, dtype=jnp.int32)[None, :]).astype(jnp.int32)
    rank_within = lax.optimization_barrier(jnp.sum((jnp.cumsum(group_match, axis=0) - group_match) * group_match, axis=1)).astype(jnp.int32)
    slots_per_group = CAP * N_EP * N_TP
    row_table = jnp.full((N_EP, slots_per_group), count_rows, jnp.int32).at[group_ids, rank_within].set(jnp.arange(count_rows, dtype=jnp.int32))
    padded_rows = jnp.concatenate([normed, jnp.zeros((1, model_width), jnp.bfloat16)], axis=0)
    padded_weights = jnp.concatenate([mix_weights, jnp.zeros((1, GROUP), jnp.float32)], axis=0)

    def one_group(group_index):
        row_index = row_table[group_index]
        rows_in = padded_rows[row_index]
        weights_in = padded_weights[row_index]
        combined = jnp.zeros((slots_per_group, model_width), jnp.float32)
        for member in range(GROUP):
            expert_index = group_index * GROUP + member
            gate_part = jnp.dot(rows_in, w_gate[expert_index], preferred_element_type=jnp.float32)
            up_part = jnp.dot(rows_in, w_up[expert_index], preferred_element_type=jnp.float32)
            hidden = (jax.nn.silu(gate_part) * up_part).astype(jnp.bfloat16)
            outputs = jnp.dot(hidden, w_down[expert_index], preferred_element_type=jnp.float32).astype(jnp.bfloat16)
            combined = combined + weights_in[:, member:member + 1] * outputs.astype(jnp.float32)
        return combined.astype(jnp.bfloat16)
    results = lax.map(one_group, jnp.arange(N_EP, dtype=jnp.int32))
    table_out = jnp.zeros((count_rows + 1, model_width), jnp.bfloat16).at[row_table.reshape(-1)].set(results.reshape(-1, model_width))
    return table_out[:count_rows]

def reference(queries, keys, values, cum_gates, expert_in, norm_gain, route_group, route_member, route_weight, w_gate, w_up, w_down):
    attended = attention_part(queries, keys, values, cum_gates)
    expert_out = expert_part(expert_in, norm_gain, route_group, route_member, route_weight, w_gate, w_up, w_down)
    return (attended, expert_out)
```

```python
import jax
import jax.numpy as jnp
from jax import lax
from jax.experimental import pallas as pl
from jax.experimental.pallas import tpu as pltpu
from jax.sharding import PartitionSpec as P

BF = jnp.bfloat16
F32 = jnp.float32
D = 4096
HALF = D // 2
FF = 384
HEAD = 128
HEADS = 4
ROWS = 128
CAP = 3
NZ, NX, NC = 8, 4, 2
NEP = 64
CHUNKS = 4
SLOTS = 48
MSG = CAP * 32
ORDER = (1, 7, 2, 5, 3, 4, 0, 6)
NEGATIVE = -1e30
EPSILON = 1e-06
SCALE = HEAD ** -0.5
Y_COPIES = 11


def dot(a, b):
    return jnp.dot(a, b, preferred_element_type=F32)


def iota(shape, dim):
    return lax.broadcasted_iota(jnp.int32, shape, dim)


def to_slots(read, store, perm_ref):
    columns = []
    for b in range(3):
        columns.append(
            jnp.concatenate([read(b, k) for k in range(32)], axis=0)
        )
    block = jnp.concatenate(columns, axis=1)
    for part in range(4):
        out = dot(perm_ref[part * 128 : (part + 1) * 128, :], block).astype(BF)
        for b in range(3):
            store(b * 512 + part * 128, out[:, b * 128 : (b + 1) * 128])


def from_slots(read, store, perm_ref):
    block = jnp.concatenate([read(b) for b in range(3)], axis=1)
    for part in range(4):
        out = dot(perm_ref[part * 128 : (part + 1) * 128, :], block).astype(BF)
        for i in range(8):
            for b in range(3):
                store(b, part * 8 + i, out[i * 16 : (i + 1) * 16, b * 128 : (b + 1) * 128])


def kernel(
    q_ref,
    keys_ref,
    values_ref,
    gates_ref,
    gates_t_ref,
    x_hbm,
    gain_ref,
    group_ref,
    member_ref,
    weight_ref,
    wg_hbm,
    wu_hbm,
    wd_hbm,
    att_ref,
    out_ref,
    x_ref,
    normed,
    gath,
    pick,
    place,
    perm_in,
    perm_out,
    send,
    recv,
    wsend,
    wrecv,
    xg,
    wgat,
    part,
    ra,
    rb,
    fl,
    fr,
    mixed,
    back,
    ret,
    total,
    hidden,
    wg,
    wu,
    wd,
    staged,
    kv,
    ga,
    load_sem,
    disp_send,
    disp_recv,
    w_send,
    w_recv,
    back_send,
    back_recv,
    kv_send,
    kv_recv,
    y_send,
    y_recv,
):
    me = lax.axis_index("ep")
    tp = lax.axis_index("tp")
    z = me // (NX * NC)
    xc = me % (NX * NC)
    x = xc // NC
    cc = xc % NC
    partner = me + 1 - 2 * cc
    right, left = (tp + 1) % 4, (tp + 3) % 4

    def ep_dev(e):
        return {"ep": e, "tp": tp}

    def tp_dev(t):
        return {"ep": me, "tp": t}

    barrier = pltpu.get_barrier_semaphore()

    @pl.loop(1, NEP)
    def _(i):
        pl.semaphore_signal(
            barrier, inc=1, device_id=ep_dev((me + i) % NEP), device_id_type=pl.DeviceIdType.MESH
        )

    for t in (right, left):
        pl.semaphore_signal(
            barrier, inc=1, device_id=tp_dev(t), device_id_type=pl.DeviceIdType.MESH
        )

    loads = [
        pltpu.make_async_copy(x_hbm, x_ref, load_sem.at[0]),
        pltpu.make_async_copy(keys_ref, staged.at[0], load_sem.at[1]),
        pltpu.make_async_copy(values_ref, staged.at[1], load_sem.at[2]),
        pltpu.make_async_copy(gates_t_ref, ga.at[z, xc], load_sem.at[3]),
        pltpu.make_async_copy(wg_hbm, wg, load_sem.at[4]),
        pltpu.make_async_copy(wu_hbm, wu, load_sem.at[5]),
        pltpu.make_async_copy(wd_hbm, wd, load_sem.at[6]),
    ]
    for c in loads:
        c.start()

    row, col = iota((512, 512), 0), iota((512, 512), 1)
    perm_in[...] = jnp.where((row & 31) * 16 + (row >> 5) == col, 1.0, 0.0).astype(BF)
    perm_out[...] = jnp.where((col & 31) * 16 + (col >> 5) == row, 1.0, 0.0).astype(BF)

    gid = group_ref[...]
    gz, gxc = gid >> 3, gid & 7
    gx, gc = gxc >> 1, gxc & 1
    dz, dx, dc = (gz - z) & 7, (gx - x) & 3, (gc + cc) & 1
    place_z = jnp.zeros_like(gid)
    for i, distance in enumerate(ORDER):
        place_z = place_z + jnp.where(dz == distance, i, 0)
    position = place_z * 8 + dx * 2 + dc
    lanes = iota((ROWS, ROWS), 1)
    match = jnp.where(position == lanes, 1.0, 0.0)
    below = jnp.where(iota((ROWS, ROWS), 0) > lanes, 1.0, 0.0).astype(BF)
    rank = jnp.sum(dot(below, match.astype(BF)) * match, axis=1, keepdims=True).astype(jnp.int32)
    slot = position * CAP + rank
    slots = jnp.where(slot == iota((ROWS, 256), 1), 1.0, 0.0)
    pick[...] = jnp.transpose(slots)[: CHUNKS * SLOTS].astype(BF)
    for c in range(CHUNKS):
        place[c] = jnp.where(slot - c * SLOTS == iota((ROWS, SLOTS), 1), 1.0, 0.0).astype(BF)
    lined = jnp.zeros((ROWS, ROWS), F32)
    for k in range(2):
        lane = rank * 4 + member_ref[:, k : k + 1]
        lined = lined + jnp.where(
            lanes == lane, weight_ref[:, k : k + 1].astype(BF).astype(F32), 0.0
        )
    wsend[...] = dot(jnp.transpose(match)[:NEP].astype(BF), lined.astype(BF)).reshape(NEP, 1, 128)

    loads[0].wait()

    @pl.loop(0, ROWS // 16)
    def _(i):
        at = pl.ds(pl.multiple_of(i * 16, 16), 16)
        floats = x_ref[at, :].astype(F32)
        mean = jnp.mean(floats * floats, axis=1, keepdims=True)
        normed[at, :] = (floats * lax.rsqrt(mean + EPSILON) * gain_ref[...]).astype(BF)

    @pl.loop(0, D // 512)
    def _(i):
        at = pl.ds(pl.multiple_of(i * 512, 512), 512)
        gath[:, at] = dot(pick[...], normed[:, at]).astype(BF)

    for c in loads[1:4]:
        c.wait()
    own = pltpu.make_async_copy(staged.at[cc], kv.at[cc, z, xc], load_sem.at[7])
    own.start()
    pl.semaphore_wait(barrier, NEP + 1)

    def remote(src, dst, ssem, rsem, dev):
        return pltpu.make_async_remote_copy(
            src_ref=src,
            dst_ref=dst,
            send_sem=ssem,
            recv_sem=rsem,
            device_id=dev,
            device_id_type=pl.DeviceIdType.MESH,
        )

    def wait_bytes(ref, sem):
        pltpu.make_async_copy(ref, ref, sem).wait()

    remote(
        staged.at[1 - cc], kv.at[1 - cc, z, xc], kv_send.at[0], kv_recv.at[0], ep_dev(partner)
    ).start()
    remote(ga.at[z, xc], ga.at[z, xc], kv_send.at[1], kv_recv.at[1], ep_dev(partner)).start()

    def message(p):
        return pl.ds(pl.multiple_of(p * MSG, MSG), MSG)

    def place_of(zi, j):
        dz = ORDER[zi]
        return (((z + dz) % NZ) * NX + (x + j // 2) % NX) * NC + (cc + j) % 2

    def place_from(zi, j):
        dz = ORDER[zi]
        return (((z + NZ - dz) % NZ) * NX + (x + NX - j // 2) % NX) * NC + (cc + j) % 2

    def for_partners(c, body):
        for zi in (2 * c, 2 * c + 1):

            @pl.loop(1 if ORDER[zi] == 0 else 0, 8)
            def _(j):
                body(zi, j, zi * 8 + j)

    own_place = ORDER.index(0) * 8
    own_chunk = own_place // 16
    own_rows = pl.ds(own_place * MSG, MSG)

    for c in range(CHUNKS):

        def read(b, k):
            return gath[c * SLOTS + b * 16 : c * SLOTS + (b + 1) * 16, k * 128 : (k + 1) * 128]

        def store(at, value):
            send[c * 1536 + at : c * 1536 + at + 128, :] = value

        to_slots(read, store, perm_in)

        def go(zi, j, p):
            remote(
                send.at[message(p)],
                recv.at[message(p)],
                disp_send,
                disp_recv.at[c],
                ep_dev(place_of(zi, j)),
            ).start()
            remote(
                wsend.at[p], wrecv.at[p], w_send, w_recv.at[c], ep_dev(place_of(zi, j))
            ).start()

        for_partners(c, go)
    pltpu.make_async_copy(send.at[own_rows], recv.at[own_rows], disp_recv.at[own_chunk]).start()
    pltpu.make_async_copy(
        wsend.at[own_place], wrecv.at[own_place], w_recv.at[own_chunk]
    ).start()

    own.wait()
    wait_bytes(staged.at[0], kv_recv.at[0])
    wait_bytes(ga.at[0, 0], kv_recv.at[1])
    pair = pl.ds(x * 2, 2)
    for dz in range(1, NZ):
        dev = ep_dev((me + dz * NX * NC) % NEP)
        remote(
            kv.at[cc, z, pair], kv.at[cc, z, pair], kv_send.at[2], kv_recv.at[2], dev
        ).start()
        remote(ga.at[z, pair], ga.at[z, pair], kv_send.at[3], kv_recv.at[3], dev).start()

    y_copies = {}

    def y_copy(c, i, src, dst, t):
        copy = remote(
            src, dst, y_send.at[c * Y_COPIES + i], y_recv.at[c * Y_COPIES + i], tp_dev(t)
        )
        copy.start()
        y_copies[c, i] = copy

    low, high = pl.ds(0, HALF), pl.ds(HALF, HALF)

    def gather_first(c):
        wait_bytes(recv.at[pl.ds(c * 1536, 1536)], disp_recv.at[c])
        wait_bytes(wrecv.at[pl.ds(c * 16, 16)], w_recv.at[c])

        def read(b):
            return recv[c * 1536 + b * 512 : c * 1536 + (b + 1) * 512, :]

        def store(b, k, value):
            xg[c, 0, b * 16 : (b + 1) * 16, k * 128 : (k + 1) * 128] = value

        from_slots(read, store, perm_out)
        wgat[c, 0] = wrecv[c * 16 : (c + 1) * 16]
        y_copy(c, 0, xg.at[c, 0], xg.at[c, 1], right)
        y_copy(c, 1, xg.at[c, 0], xg.at[c, 2], left)
        y_copy(c, 2, wgat.at[c, 0], wgat.at[c, 1], right)
        y_copy(c, 3, wgat.at[c, 0], wgat.at[c, 2], left)

    def gather_second(c):
        for i in range(4):
            y_copies[c, i].wait_recv()
        y_copy(c, 4, xg.at[c, 1, :, low], xg.at[c, 3, :, low], right)
        y_copy(c, 5, xg.at[c, 2, :, high], xg.at[c, 3, :, high], left)
        y_copy(c, 6, wgat.at[c, 1], wgat.at[c, 3], right)

    def experts(c):
        for i in range(4, 7):
            y_copies[c, i].wait_recv()
        rows = xg[c].reshape(4 * SLOTS, D)
        gate = dot(rows, wg[...])
        up = dot(rows, wu[...])
        hidden[...] = (gate / (1.0 + jnp.exp(-gate)) * up).astype(BF)
        i, j = iota((4 * SLOTS, 64), 0), iota((4 * SLOTS, 64), 1)
        spread = jnp.zeros((4 * SLOTS, 64), F32)
        for r in range(CAP):
            spread = spread + jnp.where(i == j * CAP + r, 1.0, 0.0)
        weights = dot(spread.astype(BF), wgat[c].reshape(64, 128).astype(BF))
        i, j = iota((4 * SLOTS, 128), 0), iota((4 * SLOTS, 128), 1)
        third = (i * 21846) >> 16
        mine = jnp.where(j == (i - third * CAP) * 4 + tp, weights, 0.0)
        column = jnp.sum(mine, axis=1, keepdims=True)

        @pl.loop(0, D // 512)
        def _(n):
            at = pl.ds(pl.multiple_of(n * 512, 512), 512)
            y = dot(hidden[...], wd[:, at]).astype(BF).astype(F32)
            part[c, :, :, at] = (y * column).astype(BF).reshape(4, SLOTS, 512)

        y_copy(c, 7, part.at[c, 3, :, low], ra.at[c], right)
        y_copy(c, 8, part.at[c, 3, :, high], rb.at[c], left)

    def reduce_second(c):
        y_copies[c, 7].wait_recv()
        y_copies[c, 8].wait_recv()

        @pl.loop(0, HALF // 512)
        def _(n):
            at = pl.ds(pl.multiple_of(n * 512, 512), 512)
            then = pl.ds(pl.multiple_of(n * 512 + HALF, 512), 512)
            part[c, 2, :, at] = (
                part[c, 2, :, at].astype(F32) + ra[c, :, at].astype(F32)
            ).astype(BF)
            part[c, 1, :, then] = (
                part[c, 1, :, then].astype(F32) + rb[c, :, at].astype(F32)
            ).astype(BF)

        y_copy(c, 9, part.at[c, 2], fl.at[c], right)
        y_copy(c, 10, part.at[c, 1], fr.at[c], left)

    def give_back(c):
        y_copies[c, 9].wait_recv()
        y_copies[c, 10].wait_recv()

        @pl.loop(0, D // 512)
        def _(n):
            at = pl.ds(pl.multiple_of(n * 512, 512), 512)
            mixed[:, at] = (
                part[c, 0, :, at].astype(F32)
                + fl[c, :, at].astype(F32)
                + fr[c, :, at].astype(F32)
            ).astype(BF)

        def read(b, k):
            return mixed[b * 16 : (b + 1) * 16, k * 128 : (k + 1) * 128]

        def store(at, value):
            back[c * 1536 + at : c * 1536 + at + 128, :] = value

        to_slots(read, store, perm_in)

        def go(zi, j, p):
            remote(
                back.at[message(p)],
                ret.at[message(p)],
                back_send,
                back_recv.at[c],
                ep_dev(place_from(zi, j)),
            ).start()

        for_partners(c, go)
        if c == own_chunk:
            pltpu.make_async_copy(
                back.at[own_rows], ret.at[own_rows], back_recv.at[own_chunk]
            ).start()

    def finish(c):
        wait_bytes(ret.at[pl.ds(c * 1536, 1536)], back_recv.at[c])

        def read(b):
            return ret[c * 1536 + b * 512 : c * 1536 + (b + 1) * 512, :]

        def store(b, k, value):
            mixed[b * 16 : (b + 1) * 16, k * 128 : (k + 1) * 128] = value

        from_slots(read, store, perm_out)

        @pl.loop(0, D // 512)
        def _(n):
            at = pl.ds(pl.multiple_of(n * 512, 512), 512)
            y = dot(place[c], mixed[:, at])
            if c > 0:
                y = y + total[:, at]
            if c < CHUNKS - 1:
                total[:, at] = y
            else:
                out_ref[:, at] = y.astype(BF)

    def attend(h):
        q = q_ref[:, h * HEAD : (h + 1) * HEAD]
        gate_q = gates_ref[:, h : h + 1]

        def step(kb, carried, masked):
            running, norm, acc = carried
            zi = kb // 2
            half = pl.ds((kb % 2) * 4, 4)
            k = kv[0, zi, half].reshape(512, HEAD)
            v = kv[1, zi, half].reshape(512, HEAD)
            gate_k = jnp.concatenate(
                [ga[zi, (kb % 2) * 4 + i, h : h + 1, :] for i in range(4)], axis=1
            )
            s = lax.dot_general(q, k, (((1,), (1,)), ((), ())), preferred_element_type=F32)
            s = s * SCALE + (gate_q - gate_k)
            if masked:
                allowed = iota((ROWS, 512), 1) + kb * 512 <= iota((ROWS, 512), 0) + me * ROWS
                s = jnp.where(allowed, s, NEGATIVE)
            top = jnp.maximum(running, jnp.max(s, axis=1, keepdims=True))
            w = jnp.exp(s - top)
            if masked:
                w = jnp.where(allowed, w, 0.0)
            factor = jnp.exp(running - top)
            norm = norm * factor + jnp.sum(w, axis=1, keepdims=True)
            acc = acc * factor + dot(w.astype(BF), v)
            return top, norm, acc

        carried = (
            jnp.full((ROWS, 1), NEGATIVE, F32),
            jnp.zeros((ROWS, 1), F32),
            jnp.zeros((ROWS, HEAD), F32),
        )
        last = me // 4
        carried = lax.fori_loop(0, last, lambda kb, s: step(kb, s, False), carried)
        _, norm, acc = step(last, carried, True)
        att_ref[:, h * HEAD : (h + 1) * HEAD] = (acc / norm).astype(BF)

    gather_first(0)

    wait_bytes(kv.at[0, pl.ds(0, 7), pl.ds(0, 2)], kv_recv.at[2])
    wait_bytes(ga.at[pl.ds(0, 7), pl.ds(0, 2)], kv_recv.at[3])
    for dx in range(1, NX):
        dev = ep_dev((z * NX + (x + dx) % NX) * NC + cc)
        remote(
            kv.at[cc, :, pair], kv.at[cc, :, pair], kv_send.at[4], kv_recv.at[4], dev
        ).start()
        remote(ga.at[:, pair], ga.at[:, pair], kv_send.at[5], kv_recv.at[5], dev).start()

    gather_first(1)
    gather_second(0)

    wait_bytes(kv.at[0, :, pl.ds(0, 6)], kv_recv.at[4])
    wait_bytes(ga.at[:, pl.ds(0, 6)], kv_recv.at[5])
    remote(kv.at[cc], kv.at[cc], kv_send.at[6], kv_recv.at[6], ep_dev(partner)).start()

    gather_first(2)
    for c in loads[4:7]:
        c.wait()
    experts(0)
    gather_second(1)
    wait_bytes(kv.at[0], kv_recv.at[6])
    attend(0)
    gather_first(3)
    reduce_second(0)
    experts(1)
    gather_second(2)
    attend(1)
    give_back(0)
    reduce_second(1)
    experts(2)
    gather_second(3)
    attend(2)
    reduce_second(2)
    give_back(1)
    experts(3)
    attend(3)
    give_back(2)
    reduce_second(3)
    finish(0)
    finish(1)
    give_back(3)
    finish(2)
    finish(3)

    for copy in y_copies.values():
        copy.wait_send()
    sent = pl.ds(0, (NEP - 1) * MSG)
    wait_bytes(send.at[sent], disp_send)
    wait_bytes(back.at[sent], back_send)
    wait_bytes(wsend.at[pl.ds(0, NEP - 1)], w_send)
    wait_bytes(staged.at[0], kv_send.at[0])
    wait_bytes(ga.at[0, 0], kv_send.at[1])
    wait_bytes(kv.at[0, pl.ds(0, 7), pl.ds(0, 2)], kv_send.at[2])
    wait_bytes(ga.at[pl.ds(0, 7), pl.ds(0, 2)], kv_send.at[3])
    wait_bytes(kv.at[0, :, pl.ds(0, 6)], kv_send.at[4])
    wait_bytes(ga.at[:, pl.ds(0, 6)], kv_send.at[5])
    wait_bytes(kv.at[0], kv_send.at[6])


def per_device(
    queries,
    keys,
    values,
    cum_gates,
    expert_in,
    norm_gain,
    route_group,
    route_member,
    route_weight,
    w_gate,
    w_up,
    w_down,
):
    vmem = pl.BlockSpec(memory_space=pltpu.VMEM)
    hbm = pl.BlockSpec(memory_space=pl.ANY)
    sem = pltpu.SemaphoreType.DMA
    scratch = [
        pltpu.VMEM((ROWS, D), BF),
        pltpu.VMEM((ROWS, D), BF),
        pltpu.VMEM((CHUNKS * SLOTS, D), BF),
        pltpu.VMEM((CHUNKS * SLOTS, ROWS), BF),
        pltpu.VMEM((CHUNKS, ROWS, SLOTS), BF),
        pltpu.VMEM((512, 512), BF),
        pltpu.VMEM((512, 512), BF),
        pltpu.VMEM((NEP * MSG, 128), BF),
        pltpu.VMEM((NEP * MSG, 128), BF),
        pltpu.VMEM((NEP, 1, 128), F32),
        pltpu.VMEM((NEP, 1, 128), F32),
        pltpu.VMEM((CHUNKS, 4, SLOTS, D), BF),
        pltpu.VMEM((CHUNKS, 4, 16, 1, 128), F32),
        pltpu.VMEM((CHUNKS, 4, SLOTS, D), BF),
        pltpu.VMEM((CHUNKS, SLOTS, HALF), BF),
        pltpu.VMEM((CHUNKS, SLOTS, HALF), BF),
        pltpu.VMEM((CHUNKS, SLOTS, D), BF),
        pltpu.VMEM((CHUNKS, SLOTS, D), BF),
        pltpu.VMEM((SLOTS, D), BF),
        pltpu.VMEM((NEP * MSG, 128), BF),
        pltpu.VMEM((NEP * MSG, 128), BF),
        pltpu.VMEM((ROWS, D), F32),
        pltpu.VMEM((4 * SLOTS, FF), BF),
        pltpu.VMEM((D, FF), BF),
        pltpu.VMEM((D, FF), BF),
        pltpu.VMEM((FF, D), BF),
        pltpu.VMEM((2, ROWS, HEAD), BF),
        pltpu.VMEM((2, NZ, NX * NC, ROWS, HEAD), BF),
        pltpu.VMEM((NZ, NX * NC, HEADS, ROWS), F32),
        sem((8,)),
        sem,
        sem((CHUNKS,)),
        sem,
        sem((CHUNKS,)),
        sem,
        sem((CHUNKS,)),
        sem((7,)),
        sem((7,)),
        sem((CHUNKS * Y_COPIES,)),
        sem((CHUNKS * Y_COPIES,)),
    ]
    return pl.pallas_call(
        kernel,
        name="step",
        out_shape=(
            jax.ShapeDtypeStruct((ROWS, HEADS * HEAD), BF),
            jax.ShapeDtypeStruct((ROWS, D), BF),
        ),
        in_specs=[vmem, hbm, hbm, vmem, hbm, hbm, vmem, vmem, vmem, vmem, hbm, hbm, hbm],
        out_specs=(vmem, vmem),
        scratch_shapes=scratch,
        compiler_params=pltpu.CompilerParams(
            collective_id=0, has_side_effects=True, vmem_limit_bytes=60 * 1024 * 1024
        ),
    )(
        queries,
        keys,
        values,
        cum_gates,
        cum_gates.T,
        expert_in,
        norm_gain.reshape(1, D),
        route_group,
        route_member,
        route_weight,
        w_gate[0],
        w_up[0],
        w_down[0],
    )


def solution(mesh):
    return jax.shard_map(
        per_device,
        mesh=mesh,
        in_specs=(
            P("ep", "tp"),
            P("ep", "tp"),
            P("ep", "tp"),
            P("ep", "tp"),
            P(("ep", "tp"), None),
            P(),
            P(("ep", "tp"), None),
            P(("ep", "tp"), None),
            P(("ep", "tp"), None),
            P(("ep", "tp"), None, None),
            P(("ep", "tp"), None, None),
            P(("ep", "tp"), None, None),
        ),
        out_specs=(P("ep", "tp"), P(("ep", "tp"), None)),
        check_vma=False,
    )
```

```python
import jax
import jax.numpy as jnp
from jax import lax
from jax.experimental import pallas as pl
from jax.experimental.pallas import tpu as pltpu
from jax.sharding import PartitionSpec as P

BF = jnp.bfloat16
F32 = jnp.float32
D = 4096
HALF = D // 2
FF = 384
HEAD = 128
HEADS = 4
ROWS = 128
KEYS = 2048
CAP = 3
NZ, NX, NC = 8, 4, 2
NEP = 64
CHUNKS = 4
SLOTS = 48
LINES = 16
MSG = CAP * LINES
BLOCK = 16 * LINES
PART = 16 * MSG
ORDER = (1, 7, 3, 5, 2, 6, 0, 4)
NEGATIVE = -1e30
EPSILON = 1e-06
SCALE = HEAD ** -0.5
Y_COPIES = 15


def dot(a, b):
    return jnp.dot(a, b, preferred_element_type=F32)


def iota(shape, dim):
    return lax.broadcasted_iota(jnp.int32, shape, dim)


def to_slots(read, store, perm_ref):
    columns = []
    for b in range(3):
        columns.append(jnp.concatenate([read(b, k) for k in range(LINES)], axis=0))
    block = jnp.concatenate(columns, axis=1)
    for i in range(2):
        out = dot(perm_ref[i * 128 : (i + 1) * 128, :], block).astype(BF)
        for b in range(3):
            store(b * BLOCK + i * 128, out[:, b * 128 : (b + 1) * 128])


def from_slots(read, store, perm_ref):
    block = jnp.concatenate([read(b) for b in range(3)], axis=1)
    for i in range(2):
        out = dot(perm_ref[i * 128 : (i + 1) * 128, :], block).astype(BF)
        for k in range(8):
            for b in range(3):
                store(b, i * 8 + k, out[k * 16 : (k + 1) * 16, b * 128 : (b + 1) * 128])


def kernel(
    q_ref,
    keys_ref,
    values_ref,
    gates_hbm,
    x_hbm,
    gain_ref,
    group_ref,
    member_ref,
    weight_ref,
    wg_hbm,
    wu_hbm,
    wd_hbm,
    att_ref,
    out_ref,
    x_ref,
    normed,
    gath,
    pick,
    place,
    perm,
    send,
    recv,
    wsend,
    wrecv,
    xg,
    wgat,
    part,
    ra,
    rb,
    fl,
    fr,
    mixed,
    back,
    ret,
    total,
    hidden,
    wg,
    wu,
    wd,
    staged,
    kv,
    ga,
    load_sem,
    disp_send,
    disp_recv,
    w_send,
    w_recv,
    back_send,
    back_recv,
    kv_send,
    kv_recv,
    y_send,
    y_recv,
):
    me = lax.axis_index("ep")
    tp = lax.axis_index("tp")
    z = me // (NX * NC)
    xc = me % (NX * NC)
    x = xc // NC
    cc = xc % NC
    partner = me + 1 - 2 * cc
    right, left = (tp + 1) % 4, (tp + 3) % 4

    def ep_dev(e):
        return {"ep": e, "tp": tp}

    def tp_dev(t):
        return {"ep": me, "tp": t}

    barrier = pltpu.get_barrier_semaphore()

    @pl.loop(1, NEP)
    def _(i):
        pl.semaphore_signal(
            barrier, inc=1, device_id=ep_dev((me + i) % NEP), device_id_type=pl.DeviceIdType.MESH
        )

    for t in (right, left):
        pl.semaphore_signal(
            barrier, inc=1, device_id=tp_dev(t), device_id_type=pl.DeviceIdType.MESH
        )

    loads = [
        pltpu.make_async_copy(x_hbm, x_ref, load_sem.at[0]),
        pltpu.make_async_copy(keys_ref, staged.at[0], load_sem.at[1]),
        pltpu.make_async_copy(values_ref, staged.at[1], load_sem.at[2]),
        pltpu.make_async_copy(gates_hbm, ga.at[z, xc], load_sem.at[3]),
        pltpu.make_async_copy(wg_hbm, wg, load_sem.at[4]),
        pltpu.make_async_copy(wu_hbm, wu, load_sem.at[5]),
        pltpu.make_async_copy(wd_hbm, wd, load_sem.at[6]),
    ]
    for c in loads:
        c.start()

    row, col = iota((BLOCK, BLOCK), 0), iota((BLOCK, BLOCK), 1)
    perm[...] = jnp.where((row & 15) * 16 + (row >> 4) == col, 1.0, 0.0).astype(BF)

    facts = jnp.concatenate(
        [
            group_ref[...].astype(F32),
            member_ref[...].astype(F32),
            weight_ref[...],
            jnp.zeros((3, ROWS), F32),
        ],
        axis=0,
    )
    facts = jnp.transpose(facts)
    gid = facts[:, 0:1].astype(jnp.int32)
    gz, gxc = gid >> 3, gid & 7
    gx, gc = gxc >> 1, gxc & 1
    dz, dx, dc = (gz - z) & 7, (gx - x) & 3, (gc + cc) & 1
    place_z = jnp.zeros_like(gid)
    for i, distance in enumerate(ORDER):
        place_z = place_z + jnp.where(dz == distance, i, 0)
    position = place_z * 8 + dx * 2 + dc
    lanes = iota((ROWS, ROWS), 1)
    match = jnp.where(position == lanes, 1.0, 0.0)
    below = jnp.where(iota((ROWS, ROWS), 0) > lanes, 1.0, 0.0).astype(BF)
    rank = jnp.sum(dot(below, match.astype(BF)) * match, axis=1, keepdims=True).astype(jnp.int32)
    slot = position * CAP + rank
    slots = jnp.where(slot == iota((ROWS, 256), 1), 1.0, 0.0)
    pick[...] = jnp.transpose(slots)[: CHUNKS * SLOTS].astype(BF)
    for c in range(CHUNKS):
        place[c] = jnp.where(slot - c * SLOTS == iota((ROWS, SLOTS), 1), 1.0, 0.0).astype(BF)
    lined = jnp.zeros((ROWS, ROWS), F32)
    for k in range(2):
        lane = (position & 7) * 16 + rank * 4 + facts[:, 1 + k : 2 + k].astype(jnp.int32)
        lined = lined + jnp.where(
            lanes == lane, facts[:, 3 + k : 4 + k].astype(BF).astype(F32), 0.0
        )
    wsend[...] = dot(jnp.transpose(match)[:NEP].astype(BF), lined.astype(BF)).reshape(NEP, 1, 128)

    loads[0].wait()

    @pl.loop(0, ROWS // 16)
    def _(i):
        at = pl.ds(pl.multiple_of(i * 16, 16), 16)
        floats = x_ref[at, :].astype(F32)
        mean = jnp.mean(floats * floats, axis=1, keepdims=True)
        normed[at, :] = (floats * lax.rsqrt(mean + EPSILON) * gain_ref[...]).astype(BF)

    @pl.loop(0, D // 512)
    def _(i):
        at = pl.ds(pl.multiple_of(i * 512, 512), 512)
        gath[:, at] = dot(pick[...], normed[:, at]).astype(BF)

    for c in loads[1:4]:
        c.wait()
    gate_columns = jnp.transpose(
        jnp.concatenate([ga[z, xc], jnp.zeros((4, ROWS), F32)], axis=0)
    )
    own = pltpu.make_async_copy(staged.at[cc], kv.at[cc, z, xc], load_sem.at[7])
    own.start()
    pl.semaphore_wait(barrier, NEP + 1)

    def remote(src, dst, ssem, rsem, dev):
        return pltpu.make_async_remote_copy(
            src_ref=src,
            dst_ref=dst,
            send_sem=ssem,
            recv_sem=rsem,
            device_id=dev,
            device_id_type=pl.DeviceIdType.MESH,
        )

    def wait_bytes(ref, sem):
        pltpu.make_async_copy(ref, ref, sem).wait()

    remote(
        staged.at[1 - cc], kv.at[1 - cc, z, xc], kv_send.at[0], kv_recv.at[0], ep_dev(partner)
    ).start()
    remote(ga.at[z, xc], ga.at[z, xc], kv_send.at[1], kv_recv.at[1], ep_dev(partner)).start()

    pair = pl.ds(x * 2, 2)

    def kv_along_z():
        own.wait()
        wait_bytes(staged.at[0], kv_recv.at[0])
        wait_bytes(ga.at[0, 0], kv_recv.at[1])
        for dz in range(1, NZ):
            dev = ep_dev((me + dz * NX * NC) % NEP)
            remote(
                kv.at[cc, z, pair], kv.at[cc, z, pair], kv_send.at[2], kv_recv.at[2], dev
            ).start()
            remote(ga.at[z, pair], ga.at[z, pair], kv_send.at[3], kv_recv.at[3], dev).start()

    def kv_along_x():
        wait_bytes(kv.at[0, pl.ds(0, 7), pl.ds(0, 2)], kv_recv.at[2])
        wait_bytes(ga.at[pl.ds(0, 7), pl.ds(0, 2)], kv_recv.at[3])
        for dx in range(1, NX):
            dev = ep_dev((z * NX + (x + dx) % NX) * NC + cc)
            remote(
                kv.at[cc, :, pair], kv.at[cc, :, pair], kv_send.at[4], kv_recv.at[4], dev
            ).start()
            remote(ga.at[:, pair], ga.at[:, pair], kv_send.at[5], kv_recv.at[5], dev).start()

    def kv_across():
        wait_bytes(kv.at[0, :, pl.ds(0, 6)], kv_recv.at[4])
        wait_bytes(ga.at[:, pl.ds(0, 6)], kv_recv.at[5])
        remote(kv.at[cc], kv.at[cc], kv_send.at[6], kv_recv.at[6], ep_dev(partner)).start()

    def message(p):
        return pl.ds(pl.multiple_of(p * MSG, MSG), MSG)

    def place_of(zi, j):
        dz = ORDER[zi]
        return (((z + dz) % NZ) * NX + (x + j // 2) % NX) * NC + (cc + j) % 2

    def place_from(zi, j):
        dz = ORDER[zi]
        return (((z + NZ - dz) % NZ) * NX + (x + NX - j // 2) % NX) * NC + (cc + j) % 2

    def for_partners(c, body):
        for zi in (2 * c, 2 * c + 1):

            @pl.loop(1 if ORDER[zi] == 0 else 0, 8)
            def _(j):
                body(zi, j, zi * 8 + j)

    own_place = ORDER.index(0) * 8
    own_chunk = own_place // 16
    own_rows = pl.ds(own_place * MSG, MSG)

    for c in range(CHUNKS):
        for h in range(2):

            def read(b, k):
                k = h * LINES + k
                return gath[c * SLOTS + b * 16 : c * SLOTS + (b + 1) * 16, k * 128 : (k + 1) * 128]

            def store(at, value):
                send[h, c * PART + at : c * PART + at + 128, :] = value

            to_slots(read, store, perm)

            def go(zi, j, p):
                remote(
                    send.at[h, message(p)],
                    recv.at[h, message(p)],
                    disp_send,
                    disp_recv.at[2 * c + h],
                    ep_dev(place_of(zi, j)),
                ).start()
                if h == 0:
                    remote(
                        wsend.at[p], wrecv.at[p], w_send, w_recv.at[c], ep_dev(place_of(zi, j))
                    ).start()

            for_partners(c, go)
        if c == 2:
            kv_along_z()
    for h in range(2):
        pltpu.make_async_copy(
            send.at[h, own_rows], recv.at[h, own_rows], disp_recv.at[2 * own_chunk + h]
        ).start()
    pltpu.make_async_copy(
        wsend.at[own_place], wrecv.at[own_place], w_recv.at[own_chunk]
    ).start()

    y_copies = {}

    def y_copy(c, i, src, dst, t):
        copy = remote(
            src, dst, y_send.at[c * Y_COPIES + i], y_recv.at[c * Y_COPIES + i], tp_dev(t)
        )
        copy.start()
        y_copies[c, i] = copy

    def gather_first(c, h):
        wait_bytes(recv.at[h, pl.ds(c * PART, PART)], disp_recv.at[2 * c + h])

        def read(b):
            return recv[h, c * PART + b * BLOCK : c * PART + (b + 1) * BLOCK, :]

        def store(b, k, value):
            xg[c, h, 0, b * 16 : (b + 1) * 16, k * 128 : (k + 1) * 128] = value

        from_slots(read, store, perm)
        y_copy(c, 2 * h, xg.at[c, h, 0], xg.at[c, h, 1], right)
        y_copy(c, 2 * h + 1, xg.at[c, h, 0], xg.at[c, h, 2], left)
        if h == 1:
            wait_bytes(wrecv.at[pl.ds(c * 16, 16)], w_recv.at[c])
            wgat[c, 0] = jnp.sum(wrecv[c * 16 : (c + 1) * 16].reshape(2, 8, 128), axis=1)
            y_copy(c, 4, wgat.at[c, 0], wgat.at[c, 1], right)
            y_copy(c, 5, wgat.at[c, 0], wgat.at[c, 2], left)

    def gather_second(c, h):
        if h == 0:
            y_copies[c, 0].wait_recv()
            y_copy(c, 6, xg.at[c, 0, 1], xg.at[c, 0, 3], right)
        else:
            y_copies[c, 3].wait_recv()
            y_copy(c, 7, xg.at[c, 1, 2], xg.at[c, 1, 3], left)
            y_copies[c, 4].wait_recv()
            y_copy(c, 8, wgat.at[c, 1], wgat.at[c, 3], right)

    def experts(c):
        for i in (1, 2, 5, 6, 7, 8):
            y_copies[c, i].wait_recv()
        first = xg[c, 0].reshape(4 * SLOTS, HALF)
        second = xg[c, 1].reshape(4 * SLOTS, HALF)
        gate = dot(first, wg[:HALF, :]) + dot(second, wg[HALF:, :])
        up = dot(first, wu[:HALF, :]) + dot(second, wu[HALF:, :])
        hidden[...] = (gate / (1.0 + jnp.exp(-gate)) * up).astype(BF)
        i, j = iota((4 * SLOTS, 8), 0), iota((4 * SLOTS, 8), 1)
        spread = jnp.where((i * 2731) >> 16 == j, 1.0, 0.0).astype(BF)
        weights = dot(spread, wgat[c].reshape(8, 128).astype(BF))
        i, j = iota((4 * SLOTS, 128), 0), iota((4 * SLOTS, 128), 1)
        i = i - ((i * 2731) >> 16) * 24
        source = (i * 21846) >> 16
        lane = source * 16 + (i - source * CAP) * 4 + tp
        column = jnp.sum(jnp.where(j == lane, weights, 0.0), axis=1, keepdims=True)

        def down(h):
            @pl.loop(0, HALF // 512)
            def _(n):
                at = pl.ds(pl.multiple_of(n * 512, 512), 512)
                wide = pl.ds(pl.multiple_of(n * 512 + h * HALF, 512), 512)
                y = dot(hidden[...], wd[:, wide]).astype(BF).astype(F32)
                part[c, h, :, :, at] = (y * column).astype(BF).reshape(4, SLOTS, 512)

        down(0)
        y_copy(c, 9, part.at[c, 0, 3], ra.at[c], right)
        down(1)
        y_copy(c, 10, part.at[c, 1, 3], rb.at[c], left)
        y_copy(c, 11, part.at[c, 0, 1], fr.at[c, 0], left)

    def add_to(c, h, r, ref):
        @pl.loop(0, HALF // 512)
        def _(n):
            at = pl.ds(pl.multiple_of(n * 512, 512), 512)
            part[c, h, r, :, at] = (
                part[c, h, r, :, at].astype(F32) + ref[c, :, at].astype(F32)
            ).astype(BF)

    def reduce_second(c, h):
        y_copies[c, 9 + h].wait_recv()
        if h == 0:
            add_to(c, 0, 2, ra)
            y_copy(c, 12, part.at[c, 0, 2], fl.at[c, 0], right)
            y_copy(c, 13, part.at[c, 1, 2], fl.at[c, 1], right)
        else:
            add_to(c, 1, 1, rb)
            y_copy(c, 14, part.at[c, 1, 1], fr.at[c, 1], left)

    def give_back(c, h):
        y_copies[c, 12 + h].wait_recv()
        y_copies[c, 11 + 3 * h].wait_recv()

        @pl.loop(0, HALF // 512)
        def _(n):
            at = pl.ds(pl.multiple_of(n * 512, 512), 512)
            mixed[:, at] = (
                part[c, h, 0, :, at].astype(F32)
                + fl[c, h, :, at].astype(F32)
                + fr[c, h, :, at].astype(F32)
            ).astype(BF)

        def read(b, k):
            return mixed[b * 16 : (b + 1) * 16, k * 128 : (k + 1) * 128]

        def store(at, value):
            back[h, c * PART + at : c * PART + at + 128, :] = value

        to_slots(read, store, perm)

        def go(zi, j, p):
            remote(
                back.at[h, message(p)],
                ret.at[h, message(p)],
                back_send,
                back_recv.at[2 * c + h],
                ep_dev(place_from(zi, j)),
            ).start()

        for_partners(c, go)
        if c == own_chunk:
            pltpu.make_async_copy(
                back.at[h, own_rows], ret.at[h, own_rows], back_recv.at[2 * c + h]
            ).start()

    def finish(c, h):
        wait_bytes(ret.at[h, pl.ds(c * PART, PART)], back_recv.at[2 * c + h])

        def read(b):
            return ret[h, c * PART + b * BLOCK : c * PART + (b + 1) * BLOCK, :]

        def store(b, k, value):
            mixed[b * 16 : (b + 1) * 16, k * 128 : (k + 1) * 128] = value

        from_slots(read, store, perm)

        @pl.loop(0, HALF // 512)
        def _(n):
            at = pl.ds(pl.multiple_of(n * 512, 512), 512)
            wide = pl.ds(pl.multiple_of(n * 512 + h * HALF, 512), 512)
            y = dot(place[c], mixed[:, at])
            if c > 0:
                y = y + total[:, wide]
            if c < CHUNKS - 1:
                total[:, wide] = y
            else:
                out_ref[:, wide] = y.astype(BF)

    def attend(pair_of_heads):
        heads = (2 * pair_of_heads, 2 * pair_of_heads + 1)

        def step(kb, carried, masked):
            zs = pl.ds(kb * 2, 2)
            k = kv[0, zs].reshape(KEYS, HEAD)
            v = kv[1, zs].reshape(KEYS, HEAD)
            result = []
            for h, (running, norm, acc) in zip(heads, carried):
                q = q_ref[:, h * HEAD : (h + 1) * HEAD]
                gate_k = jnp.concatenate(
                    [ga[kb * 2 + i // 8, i % 8, h : h + 1, :] for i in range(16)], axis=1
                )
                s = lax.dot_general(q, k, (((1,), (1,)), ((), ())), preferred_element_type=F32)
                s = s * SCALE + (gate_columns[:, h : h + 1] - gate_k)
                if masked:
                    behind = me * ROWS - kb * KEYS
                    allowed = iota((ROWS, KEYS), 1) - iota((ROWS, KEYS), 0) <= behind
                    s = jnp.where(allowed, s, NEGATIVE)
                top = jnp.maximum(running, jnp.max(s, axis=1, keepdims=True))
                w = jnp.exp(s - top)
                if masked:
                    w = jnp.where(allowed, w, 0.0)
                factor = jnp.exp(running - top)
                norm = norm * factor + jnp.sum(w, axis=1, keepdims=True)
                acc = acc * factor + dot(w.astype(BF), v)
                result.append((top, norm, acc))
            return tuple(result)

        start = (
            jnp.full((ROWS, 1), NEGATIVE, F32),
            jnp.zeros((ROWS, 1), F32),
            jnp.zeros((ROWS, HEAD), F32),
        )
        last = me // 16
        carried = lax.fori_loop(0, last, lambda kb, c: step(kb, c, False), (start, start))
        for h, (_, norm, acc) in zip(heads, step(last, carried, True)):
            att_ref[:, h * HEAD : (h + 1) * HEAD] = (acc / norm).astype(BF)

    gather_first(0, 0)
    gather_first(0, 1)
    gather_second(0, 0)
    gather_second(0, 1)
    gather_first(1, 0)
    gather_first(1, 1)
    gather_first(2, 0)
    gather_first(2, 1)
    gather_second(1, 0)
    gather_second(1, 1)
    for c in loads[4:7]:
        c.wait()
    experts(0)
    gather_second(2, 0)
    gather_second(2, 1)
    experts(1)
    reduce_second(0, 0)
    gather_first(3, 0)
    kv_along_x()
    experts(2)
    reduce_second(1, 0)
    kv_across()
    gather_second(3, 0)
    give_back(0, 0)
    gather_first(3, 1)
    reduce_second(1, 1)
    gather_second(3, 1)
    reduce_second(2, 0)
    reduce_second(2, 1)
    give_back(1, 0)
    wait_bytes(kv.at[0], kv_recv.at[6])
    attend(1)
    reduce_second(0, 1)
    give_back(1, 1)
    experts(3)
    finish(0, 0)
    give_back(2, 0)
    give_back(0, 1)
    give_back(2, 1)
    reduce_second(3, 0)
    finish(1, 0)
    finish(2, 0)
    reduce_second(3, 1)
    give_back(3, 0)
    finish(0, 1)
    finish(1, 1)
    give_back(3, 1)
    finish(2, 1)
    attend(0)
    finish(3, 0)
    finish(3, 1)

    for copy in y_copies.values():
        copy.wait_send()
    sent = pl.ds(0, (NEP - 1) * MSG)
    wait_bytes(send.at[:, sent], disp_send)
    wait_bytes(back.at[:, sent], back_send)
    wait_bytes(wsend.at[pl.ds(0, NEP - 1)], w_send)
    wait_bytes(staged.at[0], kv_send.at[0])
    wait_bytes(ga.at[0, 0], kv_send.at[1])
    wait_bytes(kv.at[0, pl.ds(0, 7), pl.ds(0, 2)], kv_send.at[2])
    wait_bytes(ga.at[pl.ds(0, 7), pl.ds(0, 2)], kv_send.at[3])
    wait_bytes(kv.at[0, :, pl.ds(0, 6)], kv_send.at[4])
    wait_bytes(ga.at[:, pl.ds(0, 6)], kv_send.at[5])
    wait_bytes(kv.at[0], kv_send.at[6])


def per_device(
    queries,
    keys,
    values,
    cum_gates,
    expert_in,
    norm_gain,
    route_group,
    route_member,
    route_weight,
    w_gate,
    w_up,
    w_down,
):
    vmem = pl.BlockSpec(memory_space=pltpu.VMEM)
    hbm = pl.BlockSpec(memory_space=pl.ANY)
    sem = pltpu.SemaphoreType.DMA
    scratch = [
        pltpu.VMEM((ROWS, D), BF),
        pltpu.VMEM((ROWS, D), BF),
        pltpu.VMEM((CHUNKS * SLOTS, D), BF),
        pltpu.VMEM((CHUNKS * SLOTS, ROWS), BF),
        pltpu.VMEM((CHUNKS, ROWS, SLOTS), BF),
        pltpu.VMEM((BLOCK, BLOCK), BF),
        pltpu.VMEM((2, NEP * MSG, 128), BF),
        pltpu.VMEM((2, NEP * MSG, 128), BF),
        pltpu.VMEM((NEP, 1, 128), F32),
        pltpu.VMEM((NEP, 1, 128), F32),
        pltpu.VMEM((CHUNKS, 2, 4, SLOTS, HALF), BF),
        pltpu.VMEM((CHUNKS, 4, 2, 128), F32),
        pltpu.VMEM((CHUNKS, 2, 4, SLOTS, HALF), BF),
        pltpu.VMEM((CHUNKS, SLOTS, HALF), BF),
        pltpu.VMEM((CHUNKS, SLOTS, HALF), BF),
        pltpu.VMEM((CHUNKS, 2, SLOTS, HALF), BF),
        pltpu.VMEM((CHUNKS, 2, SLOTS, HALF), BF),
        pltpu.VMEM((SLOTS, HALF), BF),
        pltpu.VMEM((2, NEP * MSG, 128), BF),
        pltpu.VMEM((2, NEP * MSG, 128), BF),
        pltpu.VMEM((ROWS, D), F32),
        pltpu.VMEM((4 * SLOTS, FF), BF),
        pltpu.VMEM((D, FF), BF),
        pltpu.VMEM((D, FF), BF),
        pltpu.VMEM((FF, D), BF),
        pltpu.VMEM((2, ROWS, HEAD), BF),
        pltpu.VMEM((2, NZ, NX * NC, ROWS, HEAD), BF),
        pltpu.VMEM((NZ, NX * NC, HEADS, ROWS), F32),
        sem((8,)),
        sem,
        sem((2 * CHUNKS,)),
        sem,
        sem((CHUNKS,)),
        sem,
        sem((2 * CHUNKS,)),
        sem((7,)),
        sem((7,)),
        sem((CHUNKS * Y_COPIES,)),
        sem((CHUNKS * Y_COPIES,)),
    ]
    return pl.pallas_call(
        kernel,
        name="step",
        out_shape=(
            jax.ShapeDtypeStruct((ROWS, HEADS * HEAD), BF),
            jax.ShapeDtypeStruct((ROWS, D), BF),
        ),
        in_specs=[vmem, hbm, hbm, hbm, hbm, vmem, vmem, vmem, vmem, hbm, hbm, hbm],
        out_specs=(vmem, vmem),
        scratch_shapes=scratch,
        compiler_params=pltpu.CompilerParams(
            collective_id=0, has_side_effects=True, vmem_limit_bytes=60 * 1024 * 1024
        ),
    )(
        queries,
        keys,
        values,
        cum_gates.T,
        expert_in,
        norm_gain.reshape(1, D),
        route_group.T,
        route_member.T,
        route_weight.T,
        w_gate[0],
        w_up[0],
        w_down[0],
    )


def solution(mesh):
    return jax.shard_map(
        per_device,
        mesh=mesh,
        in_specs=(
            P("ep", "tp"),
            P("ep", "tp"),
            P("ep", "tp"),
            P("ep", "tp"),
            P(("ep", "tp"), None),
            P(),
            P(("ep", "tp"), None),
            P(("ep", "tp"), None),
            P(("ep", "tp"), None),
            P(("ep", "tp"), None, None),
            P(("ep", "tp"), None, None),
            P(("ep", "tp"), None, None),
        ),
        out_specs=(P("ep", "tp"), P(("ep", "tp"), None)),
        check_vma=False,
    )
```

```python
import jax
import jax.numpy as jnp
from jax import lax
from jax.experimental import pallas as pl
from jax.experimental.pallas import tpu as pltpu
from jax.sharding import PartitionSpec as P

BF = jnp.bfloat16
F32 = jnp.float32
D = 4096
HALF = D // 2
FF = 384
HEAD = 128
HEADS = 4
ROWS = 128
KEYS = 2048
CAP = 3
NZ, NX, NC = 8, 4, 2
NEP = 64
CHUNKS = 4
SLOTS = 48
LINES = 16
MSG = CAP * LINES
BLOCK = 16 * LINES
PART = 16 * MSG
ORDER = (1, 7, 3, 5, 2, 6, 0, 4)
NEGATIVE = -1e30
EPSILON = 1e-06
SCALE = HEAD ** -0.5
Y_COPIES = 15


def dot(a, b):
    return jnp.dot(a, b, preferred_element_type=F32)


def iota(shape, dim):
    return lax.broadcasted_iota(jnp.int32, shape, dim)


def to_slots(read, store, perm_ref):
    columns = []
    for b in range(3):
        columns.append(jnp.concatenate([read(b, k) for k in range(LINES)], axis=0))
    block = jnp.concatenate(columns, axis=1)
    for i in range(2):
        out = dot(perm_ref[i * 128 : (i + 1) * 128, :], block).astype(BF)
        for b in range(3):
            store(b * BLOCK + i * 128, out[:, b * 128 : (b + 1) * 128])


def from_slots(read, store, perm_ref):
    block = jnp.concatenate([read(b) for b in range(3)], axis=1)
    for i in range(2):
        out = dot(perm_ref[i * 128 : (i + 1) * 128, :], block).astype(BF)
        for k in range(8):
            for b in range(3):
                store(b, i * 8 + k, out[k * 16 : (k + 1) * 16, b * 128 : (b + 1) * 128])


def kernel(
    q_ref,
    keys_ref,
    values_ref,
    gates_hbm,
    x_hbm,
    gain_ref,
    group_ref,
    member_ref,
    weight_ref,
    wg_hbm,
    wu_hbm,
    wd_hbm,
    att_ref,
    out_ref,
    x_ref,
    normed,
    gath,
    pick,
    place,
    perm,
    send,
    recv,
    wsend,
    wrecv,
    xg,
    wgat,
    part,
    ra,
    rb,
    fl,
    fr,
    mixed,
    back,
    ret,
    total,
    hidden,
    wg,
    wu,
    wd,
    staged,
    kv,
    ga,
    load_sem,
    disp_send,
    disp_recv,
    w_send,
    w_recv,
    back_send,
    back_recv,
    kv_send,
    kv_recv,
    y_send,
    y_recv,
):
    me = lax.axis_index("ep")
    tp = lax.axis_index("tp")
    z = me // (NX * NC)
    xc = me % (NX * NC)
    x = xc // NC
    cc = xc % NC
    partner = me + 1 - 2 * cc
    right, left = (tp + 1) % 4, (tp + 3) % 4

    def ep_dev(e):
        return {"ep": e, "tp": tp}

    def tp_dev(t):
        return {"ep": me, "tp": t}

    barrier = pltpu.get_barrier_semaphore()

    @pl.loop(1, NEP)
    def _(i):
        pl.semaphore_signal(
            barrier, inc=1, device_id=ep_dev((me + i) % NEP), device_id_type=pl.DeviceIdType.MESH
        )

    for t in (right, left):
        pl.semaphore_signal(
            barrier, inc=1, device_id=tp_dev(t), device_id_type=pl.DeviceIdType.MESH
        )

    loads = [
        pltpu.make_async_copy(x_hbm, x_ref, load_sem.at[0]),
        pltpu.make_async_copy(keys_ref, staged.at[0], load_sem.at[1]),
        pltpu.make_async_copy(values_ref, staged.at[1], load_sem.at[2]),
        pltpu.make_async_copy(gates_hbm, ga.at[z, xc], load_sem.at[3]),
        pltpu.make_async_copy(wg_hbm, wg, load_sem.at[4]),
        pltpu.make_async_copy(wu_hbm, wu, load_sem.at[5]),
        pltpu.make_async_copy(wd_hbm, wd, load_sem.at[6]),
    ]
    for c in loads:
        c.start()

    row, col = iota((BLOCK, BLOCK), 0), iota((BLOCK, BLOCK), 1)
    perm[...] = jnp.where((row & 15) * 16 + (row >> 4) == col, 1.0, 0.0).astype(BF)

    facts = jnp.concatenate(
        [
            group_ref[...].astype(F32),
            member_ref[...].astype(F32),
            weight_ref[...],
            jnp.zeros((3, ROWS), F32),
        ],
        axis=0,
    )
    facts = jnp.transpose(facts)
    gid = facts[:, 0:1].astype(jnp.int32)
    gz, gxc = gid >> 3, gid & 7
    gx, gc = gxc >> 1, gxc & 1
    dz, dx, dc = (gz - z) & 7, (gx - x) & 3, (gc + cc) & 1
    place_z = jnp.zeros_like(gid)
    for i, distance in enumerate(ORDER):
        place_z = place_z + jnp.where(dz == distance, i, 0)
    position = place_z * 8 + dx * 2 + dc
    lanes = iota((ROWS, ROWS), 1)
    match = jnp.where(position == lanes, 1.0, 0.0)
    below = jnp.where(iota((ROWS, ROWS), 0) > lanes, 1.0, 0.0).astype(BF)
    rank = jnp.sum(dot(below, match.astype(BF)) * match, axis=1, keepdims=True).astype(jnp.int32)
    slot = position * CAP + rank
    slots = jnp.where(slot == iota((ROWS, 256), 1), 1.0, 0.0)
    pick[...] = jnp.transpose(slots)[: CHUNKS * SLOTS].astype(BF)
    for c in range(CHUNKS):
        place[c] = jnp.where(slot - c * SLOTS == iota((ROWS, SLOTS), 1), 1.0, 0.0).astype(BF)
    lined = jnp.zeros((ROWS, ROWS), F32)
    for k in range(2):
        lane = (position & 7) * 16 + rank * 4 + facts[:, 1 + k : 2 + k].astype(jnp.int32)
        lined = lined + jnp.where(
            lanes == lane, facts[:, 3 + k : 4 + k].astype(BF).astype(F32), 0.0
        )
    wsend[...] = dot(jnp.transpose(match)[:NEP].astype(BF), lined.astype(BF)).reshape(NEP, 1, 128)

    loads[0].wait()

    @pl.loop(0, ROWS // 16, unroll=4)
    def _(i):
        at = pl.ds(pl.multiple_of(i * 16, 16), 16)
        floats = x_ref[at, :].astype(F32)
        mean = jnp.mean(floats * floats, axis=1, keepdims=True)
        normed[at, :] = (floats * lax.rsqrt(mean + EPSILON) * gain_ref[...]).astype(BF)

    def gather_rows(c):
        rows = pl.ds(c * SLOTS, SLOTS)

        @pl.loop(0, D // 512, unroll=2)
        def _(i):
            at = pl.ds(pl.multiple_of(i * 512, 512), 512)
            gath[rows, at] = dot(pick[rows, :], normed[:, at]).astype(BF)

        for h in range(2):

            def read(b, k):
                k = h * LINES + k
                return gath[c * SLOTS + b * 16 : c * SLOTS + (b + 1) * 16, k * 128 : (k + 1) * 128]

            def store(at, value):
                send[h, c * PART + at : c * PART + at + 128, :] = value

            to_slots(read, store, perm)

    gather_rows(0)
    for c in loads[1:4]:
        c.wait()
    own = pltpu.make_async_copy(staged.at[cc], kv.at[cc, z, xc], load_sem.at[7])
    own.start()
    pl.semaphore_wait(barrier, NEP + 1)

    def remote(src, dst, ssem, rsem, dev):
        return pltpu.make_async_remote_copy(
            src_ref=src,
            dst_ref=dst,
            send_sem=ssem,
            recv_sem=rsem,
            device_id=dev,
            device_id_type=pl.DeviceIdType.MESH,
        )

    def wait_bytes(ref, sem):
        pltpu.make_async_copy(ref, ref, sem).wait()

    pair = pl.ds(x * 2, 2)

    def kv_along_z():
        own.wait()
        wait_bytes(staged.at[0], kv_recv.at[0])
        wait_bytes(ga.at[0, 0], kv_recv.at[1])
        for dz in range(1, NZ):
            dev = ep_dev((me + dz * NX * NC) % NEP)
            remote(
                kv.at[cc, z, pair], kv.at[cc, z, pair], kv_send.at[2], kv_recv.at[2], dev
            ).start()
            remote(ga.at[z, pair], ga.at[z, pair], kv_send.at[3], kv_recv.at[3], dev).start()

    def kv_along_x():
        wait_bytes(kv.at[0, pl.ds(0, 7), pl.ds(0, 2)], kv_recv.at[2])
        wait_bytes(ga.at[pl.ds(0, 7), pl.ds(0, 2)], kv_recv.at[3])
        for dx in range(1, NX):
            dev = ep_dev((z * NX + (x + dx) % NX) * NC + cc)
            remote(
                kv.at[cc, :, pair], kv.at[cc, :, pair], kv_send.at[4], kv_recv.at[4], dev
            ).start()
            remote(ga.at[:, pair], ga.at[:, pair], kv_send.at[5], kv_recv.at[5], dev).start()

    def kv_across():
        wait_bytes(kv.at[0, :, pl.ds(0, 6)], kv_recv.at[4])
        wait_bytes(ga.at[:, pl.ds(0, 6)], kv_recv.at[5])
        remote(kv.at[cc], kv.at[cc], kv_send.at[6], kv_recv.at[6], ep_dev(partner)).start()

    def message(p):
        return pl.ds(pl.multiple_of(p * MSG, MSG), MSG)

    def place_of(zi, j):
        dz = ORDER[zi]
        return (((z + dz) % NZ) * NX + (x + j // 2) % NX) * NC + (cc + j) % 2

    def place_from(zi, j):
        dz = ORDER[zi]
        return (((z + NZ - dz) % NZ) * NX + (x + NX - j // 2) % NX) * NC + (cc + j) % 2

    def for_partners(c, body):
        for zi in (2 * c, 2 * c + 1):

            @pl.loop(1 if ORDER[zi] == 0 else 0, 8)
            def _(j):
                body(zi, j, zi * 8 + j)

    own_place = ORDER.index(0) * 8
    own_chunk = own_place // 16
    own_rows = pl.ds(own_place * MSG, MSG)

    for c in range(CHUNKS):
        if c > 0:
            gather_rows(c)
        for h in range(2):

            def go(zi, j, p):
                remote(
                    send.at[h, message(p)],
                    recv.at[h, message(p)],
                    disp_send,
                    disp_recv.at[2 * c + h],
                    ep_dev(place_of(zi, j)),
                ).start()
                if h == 0:
                    remote(
                        wsend.at[p], wrecv.at[p], w_send, w_recv.at[c], ep_dev(place_of(zi, j))
                    ).start()

            for_partners(c, go)
        if c == 0:
            remote(
                staged.at[1 - cc], kv.at[1 - cc, z, xc], kv_send.at[0], kv_recv.at[0], ep_dev(partner)
            ).start()
            remote(ga.at[z, xc], ga.at[z, xc], kv_send.at[1], kv_recv.at[1], ep_dev(partner)).start()
        if c == 2:
            kv_along_z()
    for h in range(2):
        pltpu.make_async_copy(
            send.at[h, own_rows], recv.at[h, own_rows], disp_recv.at[2 * own_chunk + h]
        ).start()
    pltpu.make_async_copy(
        wsend.at[own_place], wrecv.at[own_place], w_recv.at[own_chunk]
    ).start()

    y_copies = {}

    def y_copy(c, i, src, dst, t):
        copy = remote(
            src, dst, y_send.at[c * Y_COPIES + i], y_recv.at[c * Y_COPIES + i], tp_dev(t)
        )
        copy.start()
        y_copies[c, i] = copy

    def gather_first(c, h):
        wait_bytes(recv.at[h, pl.ds(c * PART, PART)], disp_recv.at[2 * c + h])

        def read(b):
            return recv[h, c * PART + b * BLOCK : c * PART + (b + 1) * BLOCK, :]

        def store(b, k, value):
            xg[c, h, 0, b * 16 : (b + 1) * 16, k * 128 : (k + 1) * 128] = value

        from_slots(read, store, perm)
        y_copy(c, 2 * h, xg.at[c, h, 0], xg.at[c, h, 1], right)
        y_copy(c, 2 * h + 1, xg.at[c, h, 0], xg.at[c, h, 2], left)
        if h == 1:
            wait_bytes(wrecv.at[pl.ds(c * 16, 16)], w_recv.at[c])
            wgat[c, 0] = jnp.sum(wrecv[c * 16 : (c + 1) * 16].reshape(2, 8, 128), axis=1)
            y_copy(c, 4, wgat.at[c, 0], wgat.at[c, 1], right)
            y_copy(c, 5, wgat.at[c, 0], wgat.at[c, 2], left)

    def gather_second(c, h):
        if h == 0:
            y_copies[c, 0].wait_recv()
            y_copy(c, 6, xg.at[c, 0, 1], xg.at[c, 0, 3], right)
        else:
            y_copies[c, 3].wait_recv()
            y_copy(c, 7, xg.at[c, 1, 2], xg.at[c, 1, 3], left)
            y_copies[c, 4].wait_recv()
            y_copy(c, 8, wgat.at[c, 1], wgat.at[c, 3], right)

    def experts(c):
        for i in (1, 2, 5, 6, 7, 8):
            y_copies[c, i].wait_recv()
        first = xg[c, 0].reshape(4 * SLOTS, HALF)
        second = xg[c, 1].reshape(4 * SLOTS, HALF)
        gate = dot(first, wg[:HALF, :]) + dot(second, wg[HALF:, :])
        up = dot(first, wu[:HALF, :]) + dot(second, wu[HALF:, :])
        hidden[...] = (gate / (1.0 + jnp.exp(-gate)) * up).astype(BF)
        i, j = iota((4 * SLOTS, 8), 0), iota((4 * SLOTS, 8), 1)
        spread = jnp.where((i * 2731) >> 16 == j, 1.0, 0.0).astype(BF)
        weights = dot(spread, wgat[c].reshape(8, 128).astype(BF))
        i, j = iota((4 * SLOTS, 128), 0), iota((4 * SLOTS, 128), 1)
        i = i - ((i * 2731) >> 16) * 24
        source = (i * 21846) >> 16
        lane = source * 16 + (i - source * CAP) * 4 + tp
        column = jnp.sum(jnp.where(j == lane, weights, 0.0), axis=1, keepdims=True)

        def down(h):
            @pl.loop(0, HALF // 512)
            def _(n):
                at = pl.ds(pl.multiple_of(n * 512, 512), 512)
                wide = pl.ds(pl.multiple_of(n * 512 + h * HALF, 512), 512)
                y = dot(hidden[...], wd[:, wide]).astype(BF).astype(F32)
                part[c, h, :, :, at] = (y * column).astype(BF).reshape(4, SLOTS, 512)

        down(0)
        y_copy(c, 9, part.at[c, 0, 3], ra.at[c], right)
        down(1)
        y_copy(c, 10, part.at[c, 1, 3], rb.at[c], left)
        y_copy(c, 11, part.at[c, 0, 1], fr.at[c, 0], left)

    def add_to(c, h, r, ref):
        @pl.loop(0, HALF // 512)
        def _(n):
            at = pl.ds(pl.multiple_of(n * 512, 512), 512)
            part[c, h, r, :, at] = (
                part[c, h, r, :, at].astype(F32) + ref[c, :, at].astype(F32)
            ).astype(BF)

    def reduce_second(c, h):
        y_copies[c, 9 + h].wait_recv()
        if h == 0:
            add_to(c, 0, 2, ra)
            y_copy(c, 12, part.at[c, 0, 2], fl.at[c, 0], right)
            y_copy(c, 13, part.at[c, 1, 2], fl.at[c, 1], right)
        else:
            add_to(c, 1, 1, rb)
            y_copy(c, 14, part.at[c, 1, 1], fr.at[c, 1], left)

    def give_back(c, h):
        y_copies[c, 12 + h].wait_recv()
        y_copies[c, 11 + 3 * h].wait_recv()

        @pl.loop(0, HALF // 512)
        def _(n):
            at = pl.ds(pl.multiple_of(n * 512, 512), 512)
            mixed[:, at] = (
                part[c, h, 0, :, at].astype(F32)
                + fl[c, h, :, at].astype(F32)
                + fr[c, h, :, at].astype(F32)
            ).astype(BF)

        def read(b, k):
            return mixed[b * 16 : (b + 1) * 16, k * 128 : (k + 1) * 128]

        def store(at, value):
            back[h, c * PART + at : c * PART + at + 128, :] = value

        to_slots(read, store, perm)

        def go(zi, j, p):
            remote(
                back.at[h, message(p)],
                ret.at[h, message(p)],
                back_send,
                back_recv.at[2 * c + h],
                ep_dev(place_from(zi, j)),
            ).start()

        for_partners(c, go)
        if c == own_chunk:
            pltpu.make_async_copy(
                back.at[h, own_rows], ret.at[h, own_rows], back_recv.at[2 * c + h]
            ).start()

    def finish(c, h):
        wait_bytes(ret.at[h, pl.ds(c * PART, PART)], back_recv.at[2 * c + h])

        def read(b):
            return ret[h, c * PART + b * BLOCK : c * PART + (b + 1) * BLOCK, :]

        def store(b, k, value):
            mixed[b * 16 : (b + 1) * 16, k * 128 : (k + 1) * 128] = value

        from_slots(read, store, perm)

        @pl.loop(0, HALF // 512)
        def _(n):
            at = pl.ds(pl.multiple_of(n * 512, 512), 512)
            wide = pl.ds(pl.multiple_of(n * 512 + h * HALF, 512), 512)
            y = dot(place[c], mixed[:, at])
            if c > 0:
                y = y + total[:, wide]
            if c < CHUNKS - 1:
                total[:, wide] = y
            else:
                out_ref[:, wide] = y.astype(BF)

    def attend(pair_of_heads):
        heads = (2 * pair_of_heads, 2 * pair_of_heads + 1)
        gate_columns = jnp.transpose(
            jnp.concatenate([ga[z, xc], jnp.zeros((4, ROWS), F32)], axis=0)
        )

        def step(kb, carried, masked):
            zs = pl.ds(kb * 2, 2)
            k = kv[0, zs].reshape(KEYS, HEAD)
            v = kv[1, zs].reshape(KEYS, HEAD)
            result = []
            for h, (running, norm, acc) in zip(heads, carried):
                q = q_ref[:, h * HEAD : (h + 1) * HEAD]
                gate_k = jnp.concatenate(
                    [ga[kb * 2 + i // 8, i % 8, h : h + 1, :] for i in range(16)], axis=1
                )
                s = lax.dot_general(q, k, (((1,), (1,)), ((), ())), preferred_element_type=F32)
                s = s * SCALE + (gate_columns[:, h : h + 1] - gate_k)
                if masked:
                    behind = me * ROWS - kb * KEYS
                    allowed = iota((ROWS, KEYS), 1) - iota((ROWS, KEYS), 0) <= behind
                    s = jnp.where(allowed, s, NEGATIVE)
                top = jnp.maximum(running, jnp.max(s, axis=1, keepdims=True))
                w = jnp.exp(s - top)
                if masked:
                    w = jnp.where(allowed, w, 0.0)
                factor = jnp.exp(running - top)
                norm = norm * factor + jnp.sum(w, axis=1, keepdims=True)
                acc = acc * factor + dot(w.astype(BF), v)
                result.append((top, norm, acc))
            return tuple(result)

        start = (
            jnp.full((ROWS, 1), NEGATIVE, F32),
            jnp.zeros((ROWS, 1), F32),
            jnp.zeros((ROWS, HEAD), F32),
        )
        last = me // 16
        carried = lax.fori_loop(0, last, lambda kb, c: step(kb, c, False), (start, start))
        for h, (_, norm, acc) in zip(heads, step(last, carried, True)):
            att_ref[:, h * HEAD : (h + 1) * HEAD] = (acc / norm).astype(BF)

    gather_first(0, 0)
    gather_first(0, 1)
    gather_second(0, 0)
    gather_second(0, 1)
    gather_first(1, 0)
    gather_first(1, 1)
    gather_first(2, 0)
    gather_first(2, 1)
    for c in loads[4:7]:
        c.wait()
    experts(0)
    gather_second(1, 0)
    gather_second(1, 1)
    gather_second(2, 1)
    reduce_second(0, 0)
    kv_along_x()
    give_back(0, 0)
    gather_first(3, 0)
    gather_first(3, 1)
    experts(1)
    gather_second(2, 0)
    reduce_second(0, 1)
    finish(0, 0)
    reduce_second(1, 0)
    reduce_second(1, 1)
    gather_second(3, 1)
    experts(2)
    give_back(1, 0)
    gather_second(3, 0)
    give_back(0, 1)
    kv_across()
    give_back(1, 1)
    reduce_second(2, 0)
    wait_bytes(kv.at[0], kv_recv.at[6])
    attend(1)
    finish(1, 0)
    reduce_second(2, 1)
    experts(3)
    give_back(2, 0)
    give_back(2, 1)
    finish(0, 1)
    reduce_second(3, 0)
    reduce_second(3, 1)
    give_back(3, 0)
    finish(1, 1)
    finish(2, 0)
    give_back(3, 1)
    finish(2, 1)
    attend(0)
    finish(3, 0)
    finish(3, 1)

    for copy in y_copies.values():
        copy.wait_send()
    sent = pl.ds(0, (NEP - 1) * MSG)
    wait_bytes(send.at[:, sent], disp_send)
    wait_bytes(back.at[:, sent], back_send)
    wait_bytes(wsend.at[pl.ds(0, NEP - 1)], w_send)
    wait_bytes(staged.at[0], kv_send.at[0])
    wait_bytes(ga.at[0, 0], kv_send.at[1])
    wait_bytes(kv.at[0, pl.ds(0, 7), pl.ds(0, 2)], kv_send.at[2])
    wait_bytes(ga.at[pl.ds(0, 7), pl.ds(0, 2)], kv_send.at[3])
    wait_bytes(kv.at[0, :, pl.ds(0, 6)], kv_send.at[4])
    wait_bytes(ga.at[:, pl.ds(0, 6)], kv_send.at[5])
    wait_bytes(kv.at[0], kv_send.at[6])


def per_device(
    queries,
    keys,
    values,
    cum_gates,
    expert_in,
    norm_gain,
    route_group,
    route_member,
    route_weight,
    w_gate,
    w_up,
    w_down,
):
    vmem = pl.BlockSpec(memory_space=pltpu.VMEM)
    hbm = pl.BlockSpec(memory_space=pl.ANY)
    sem = pltpu.SemaphoreType.DMA
    scratch = [
        pltpu.VMEM((ROWS, D), BF),
        pltpu.VMEM((ROWS, D), BF),
        pltpu.VMEM((CHUNKS * SLOTS, D), BF),
        pltpu.VMEM((CHUNKS * SLOTS, ROWS), BF),
        pltpu.VMEM((CHUNKS, ROWS, SLOTS), BF),
        pltpu.VMEM((BLOCK, BLOCK), BF),
        pltpu.VMEM((2, NEP * MSG, 128), BF),
        pltpu.VMEM((2, NEP * MSG, 128), BF),
        pltpu.VMEM((NEP, 1, 128), F32),
        pltpu.VMEM((NEP, 1, 128), F32),
        pltpu.VMEM((CHUNKS, 2, 4, SLOTS, HALF), BF),
        pltpu.VMEM((CHUNKS, 4, 2, 128), F32),
        pltpu.VMEM((CHUNKS, 2, 4, SLOTS, HALF), BF),
        pltpu.VMEM((CHUNKS, SLOTS, HALF), BF),
        pltpu.VMEM((CHUNKS, SLOTS, HALF), BF),
        pltpu.VMEM((CHUNKS, 2, SLOTS, HALF), BF),
        pltpu.VMEM((CHUNKS, 2, SLOTS, HALF), BF),
        pltpu.VMEM((SLOTS, HALF), BF),
        pltpu.VMEM((2, NEP * MSG, 128), BF),
        pltpu.VMEM((2, NEP * MSG, 128), BF),
        pltpu.VMEM((ROWS, D), F32),
        pltpu.VMEM((4 * SLOTS, FF), BF),
        pltpu.VMEM((D, FF), BF),
        pltpu.VMEM((D, FF), BF),
        pltpu.VMEM((FF, D), BF),
        pltpu.VMEM((2, ROWS, HEAD), BF),
        pltpu.VMEM((2, NZ, NX * NC, ROWS, HEAD), BF),
        pltpu.VMEM((NZ, NX * NC, HEADS, ROWS), F32),
        sem((8,)),
        sem,
        sem((2 * CHUNKS,)),
        sem,
        sem((CHUNKS,)),
        sem,
        sem((2 * CHUNKS,)),
        sem((7,)),
        sem((7,)),
        sem((CHUNKS * Y_COPIES,)),
        sem((CHUNKS * Y_COPIES,)),
    ]
    return pl.pallas_call(
        kernel,
        name="step",
        out_shape=(
            pltpu.VMEM((ROWS, HEADS * HEAD), BF),
            pltpu.VMEM((ROWS, D), BF),
        ),
        in_specs=[vmem, hbm, hbm, hbm, hbm, vmem, vmem, vmem, vmem, hbm, hbm, hbm],
        out_specs=(vmem, vmem),
        scratch_shapes=scratch,
        compiler_params=pltpu.CompilerParams(
            collective_id=0, has_side_effects=True, vmem_limit_bytes=60 * 1024 * 1024
        ),
    )(
        queries,
        keys,
        values,
        cum_gates.T,
        expert_in,
        norm_gain.reshape(1, D),
        route_group.T,
        route_member.T,
        route_weight.T,
        w_gate[0],
        w_up[0],
        w_down[0],
    )


def solution(mesh):
    return jax.shard_map(
        per_device,
        mesh=mesh,
        in_specs=(
            P("ep", "tp"),
            P("ep", "tp"),
            P("ep", "tp"),
            P("ep", "tp"),
            P(("ep", "tp"), None),
            P(),
            P(("ep", "tp"), None),
            P(("ep", "tp"), None),
            P(("ep", "tp"), None),
            P(("ep", "tp"), None, None),
            P(("ep", "tp"), None, None),
            P(("ep", "tp"), None, None),
        ),
        out_specs=(P("ep", "tp"), P(("ep", "tp"), None)),
        check_vma=False,
    )
```

```python
import jax
import jax.numpy as jnp
from jax import lax
from jax.experimental import pallas as pl
from jax.experimental.pallas import tpu as pltpu
from jax.sharding import PartitionSpec as P

BF = jnp.bfloat16
F32 = jnp.float32
D = 4096
HALF = D // 2
FF = 384
HEAD = 128
HEADS = 4
ROWS = 128
KEYS = 2048
CAP = 3
NZ, NX, NC = 8, 4, 2
NEP = 64
CHUNKS = 4
SLOTS = 48
LINES = 16
MSG = CAP * LINES
BLOCK = 16 * LINES
PART = 16 * MSG
ORDER = (0, 6, 2, 4, 3, 5, 1, 7)
NEGATIVE = -1e30
EPSILON = 1e-06
SCALE = HEAD ** -0.5
Y_COPIES = 15


def dot(a, b):
    return jnp.dot(a, b, preferred_element_type=F32)


def iota(shape, dim):
    return lax.broadcasted_iota(jnp.int32, shape, dim)


def to_slots(read, store, perm_ref):
    columns = []
    for b in range(3):
        columns.append(jnp.concatenate([read(b, k) for k in range(LINES)], axis=0))
    block = jnp.concatenate(columns, axis=1)
    for i in range(2):
        out = dot(perm_ref[i * 128 : (i + 1) * 128, :], block).astype(BF)
        for b in range(3):
            store(b * BLOCK + i * 128, out[:, b * 128 : (b + 1) * 128])


def from_slots(read, store, perm_ref):
    block = jnp.concatenate([read(b) for b in range(3)], axis=1)
    for i in range(2):
        out = dot(perm_ref[i * 128 : (i + 1) * 128, :], block).astype(BF)
        for k in range(8):
            for b in range(3):
                store(b, i * 8 + k, out[k * 16 : (k + 1) * 16, b * 128 : (b + 1) * 128])


def kernel(
    q_hbm,
    keys_ref,
    values_ref,
    gates_hbm,
    x_hbm,
    gain_hbm,
    group_hbm,
    member_hbm,
    weight_hbm,
    wg_hbm,
    wu_hbm,
    wd_hbm,
    att_ref,
    out_ref,
    q_ref,
    gain_ref,
    group_ref,
    member_ref,
    weight_ref,
    x_ref,
    normed,
    gath,
    pick,
    place,
    perm,
    send,
    recv,
    wsend,
    wrecv,
    xg,
    wgat,
    part,
    ra,
    rb,
    fl,
    fr,
    mixed,
    back,
    ret,
    total,
    hidden,
    wg,
    wu,
    wd,
    staged,
    kv,
    ga,
    load_sem,
    disp_send,
    disp_recv,
    w_send,
    w_recv,
    back_send,
    back_recv,
    kv_send,
    kv_recv,
    y_send,
    y_recv,
):
    me = lax.axis_index("ep")
    tp = lax.axis_index("tp")
    z = me // (NX * NC)
    xc = me % (NX * NC)
    x = xc // NC
    cc = xc % NC
    partner = me + 1 - 2 * cc
    right, left = (tp + 1) % 4, (tp + 3) % 4

    def ep_dev(e):
        return {"ep": e, "tp": tp}

    def tp_dev(t):
        return {"ep": me, "tp": t}

    quarters = [pl.ds(i * 32, 32) for i in range(4)]
    x_loads = [
        pltpu.make_async_copy(x_hbm.at[at], x_ref.at[at], load_sem.at[i])
        for i, at in enumerate(quarters)
    ]
    facts_loads = [
        pltpu.make_async_copy(group_hbm, group_ref, load_sem.at[4]),
        pltpu.make_async_copy(member_hbm, member_ref, load_sem.at[5]),
        pltpu.make_async_copy(weight_hbm, weight_ref, load_sem.at[6]),
        pltpu.make_async_copy(gain_hbm, gain_ref, load_sem.at[7]),
    ]
    kv_loads = [
        pltpu.make_async_copy(keys_ref, staged.at[0], load_sem.at[8]),
        pltpu.make_async_copy(values_ref, staged.at[1], load_sem.at[9]),
        pltpu.make_async_copy(gates_hbm, ga.at[z, xc], load_sem.at[10]),
    ]
    late_loads = [
        pltpu.make_async_copy(wg_hbm, wg, load_sem.at[11]),
        pltpu.make_async_copy(wu_hbm, wu, load_sem.at[12]),
        pltpu.make_async_copy(wd_hbm, wd, load_sem.at[13]),
        pltpu.make_async_copy(q_hbm, q_ref, load_sem.at[14]),
    ]
    for copy in facts_loads + x_loads + kv_loads:
        copy.start()

    barrier = pltpu.get_barrier_semaphore()

    @pl.loop(1, NEP)
    def _(i):
        pl.semaphore_signal(
            barrier, inc=1, device_id=ep_dev((me + i) % NEP), device_id_type=pl.DeviceIdType.MESH
        )

    for t in (right, left):
        pl.semaphore_signal(
            barrier, inc=1, device_id=tp_dev(t), device_id_type=pl.DeviceIdType.MESH
        )

    row, col = iota((BLOCK, BLOCK), 0), iota((BLOCK, BLOCK), 1)
    perm[...] = jnp.where((row & 15) * 16 + (row >> 4) == col, 1.0, 0.0).astype(BF)

    for copy in facts_loads:
        copy.wait()
    facts = jnp.concatenate(
        [
            group_ref[...].astype(F32),
            member_ref[...].astype(F32),
            weight_ref[...],
            jnp.zeros((3, ROWS), F32),
        ],
        axis=0,
    )
    facts = jnp.transpose(facts)
    gid = facts[:, 0:1].astype(jnp.int32)
    gz, gxc = gid >> 3, gid & 7
    gx, gc = gxc >> 1, gxc & 1
    dz, dx, dc = (gz - z) & 7, (gx - x) & 3, (gc + cc) & 1
    place_z = jnp.zeros_like(gid)
    for i, distance in enumerate(ORDER):
        place_z = place_z + jnp.where(dz == distance, i, 0)
    position = place_z * 8 + dx * 2 + dc
    lanes = iota((ROWS, ROWS), 1)
    match = jnp.where(position == lanes, 1.0, 0.0)
    below = jnp.where(iota((ROWS, ROWS), 0) > lanes, 1.0, 0.0).astype(BF)
    rank = jnp.sum(dot(below, match.astype(BF)) * match, axis=1, keepdims=True).astype(jnp.int32)
    slot = position * CAP + rank
    slots = jnp.where(slot == iota((ROWS, 256), 1), 1.0, 0.0)
    pick[...] = jnp.transpose(slots)[: CHUNKS * SLOTS].astype(BF)
    lined = jnp.zeros((ROWS, ROWS), F32)
    for k in range(2):
        lane = (position & 7) * 16 + rank * 4 + facts[:, 1 + k : 2 + k].astype(jnp.int32)
        lined = lined + jnp.where(
            lanes == lane, facts[:, 3 + k : 4 + k].astype(BF).astype(F32), 0.0
        )
    wsend[...] = dot(jnp.transpose(match)[:NEP].astype(BF), lined.astype(BF)).reshape(NEP, 1, 128)

    for copy in x_loads:
        copy.wait()
    for copy in late_loads:
        copy.start()

    @pl.loop(0, ROWS // 16, unroll=4)
    def _(i):
        at = pl.ds(pl.multiple_of(i * 16, 16), 16)
        floats = x_ref[at, :].astype(F32)
        mean = jnp.mean(floats * floats, axis=1, keepdims=True)
        normed[at, :] = (floats * lax.rsqrt(mean + EPSILON) * gain_ref[...]).astype(BF)

    def gather_rows(c):
        rows = pl.ds(c * SLOTS, SLOTS)

        @pl.loop(0, D // 512, unroll=2)
        def _(i):
            at = pl.ds(pl.multiple_of(i * 512, 512), 512)
            gath[rows, at] = dot(pick[rows, :], normed[:, at]).astype(BF)

        for h in range(2):

            def read(b, k):
                k = h * LINES + k
                return gath[c * SLOTS + b * 16 : c * SLOTS + (b + 1) * 16, k * 128 : (k + 1) * 128]

            def store(at, value):
                send[h, c * PART + at : c * PART + at + 128, :] = value

            to_slots(read, store, perm)

    gather_rows(0)
    for copy in kv_loads:
        copy.wait()
    own = pltpu.make_async_copy(staged.at[cc], kv.at[cc, z, xc], load_sem.at[15])
    own.start()
    pl.semaphore_wait(barrier, NEP + 1)

    def remote(src, dst, ssem, rsem, dev):
        return pltpu.make_async_remote_copy(
            src_ref=src,
            dst_ref=dst,
            send_sem=ssem,
            recv_sem=rsem,
            device_id=dev,
            device_id_type=pl.DeviceIdType.MESH,
        )

    def wait_bytes(ref, sem):
        pltpu.make_async_copy(ref, ref, sem).wait()

    pair = pl.ds(x * 2, 2)

    def kv_along_z():
        own.wait()
        wait_bytes(staged.at[0], kv_recv.at[0])
        wait_bytes(ga.at[0, 0], kv_recv.at[1])
        for dz in range(1, NZ):
            dev = ep_dev((me + dz * NX * NC) % NEP)
            remote(
                kv.at[cc, z, pair], kv.at[cc, z, pair], kv_send.at[2], kv_recv.at[2], dev
            ).start()
            remote(ga.at[z, pair], ga.at[z, pair], kv_send.at[3], kv_recv.at[3], dev).start()

    def kv_along_x():
        wait_bytes(kv.at[0, pl.ds(0, 7), pl.ds(0, 2)], kv_recv.at[2])
        wait_bytes(ga.at[pl.ds(0, 7), pl.ds(0, 2)], kv_recv.at[3])
        for dx in range(1, NX):
            dev = ep_dev((z * NX + (x + dx) % NX) * NC + cc)
            remote(
                kv.at[cc, :, pair], kv.at[cc, :, pair], kv_send.at[4], kv_recv.at[4], dev
            ).start()
            remote(ga.at[:, pair], ga.at[:, pair], kv_send.at[5], kv_recv.at[5], dev).start()

    def kv_across():
        wait_bytes(kv.at[0, :, pl.ds(0, 6)], kv_recv.at[4])
        wait_bytes(ga.at[:, pl.ds(0, 6)], kv_recv.at[5])
        remote(kv.at[cc], kv.at[cc], kv_send.at[6], kv_recv.at[6], ep_dev(partner)).start()

    def message(p):
        return pl.ds(pl.multiple_of(p * MSG, MSG), MSG)

    def place_of(zi, j):
        dz = ORDER[zi]
        return (((z + dz) % NZ) * NX + (x + j // 2) % NX) * NC + (cc + j) % 2

    def place_from(zi, j):
        dz = ORDER[zi]
        return (((z + NZ - dz) % NZ) * NX + (x + NX - j // 2) % NX) * NC + (cc + j) % 2

    def for_partners(c, body):
        for zi in (2 * c, 2 * c + 1):

            @pl.loop(1 if ORDER[zi] == 0 else 0, 8)
            def _(j):
                body(zi, j, zi * 8 + j)

    own_place = ORDER.index(0) * 8
    own_chunk = own_place // 16
    own_rows = pl.ds(own_place * MSG, MSG)

    for c in range(CHUNKS):
        if c > 0:
            gather_rows(c)
        for h in range(2):

            def go(zi, j, p):
                if h == 0:
                    remote(
                        wsend.at[p], wrecv.at[p], w_send, w_recv.at[c], ep_dev(place_of(zi, j))
                    ).start()
                remote(
                    send.at[h, message(p)],
                    recv.at[h, message(p)],
                    disp_send,
                    disp_recv.at[2 * c + h],
                    ep_dev(place_of(zi, j)),
                ).start()

            for_partners(c, go)
        if c == 0:
            remote(
                staged.at[1 - cc], kv.at[1 - cc, z, xc], kv_send.at[0], kv_recv.at[0], ep_dev(partner)
            ).start()
            remote(ga.at[z, xc], ga.at[z, xc], kv_send.at[1], kv_recv.at[1], ep_dev(partner)).start()
        if c == 2:
            kv_along_z()
    for h in range(2):
        pltpu.make_async_copy(
            send.at[h, own_rows], recv.at[h, own_rows], disp_recv.at[2 * own_chunk + h]
        ).start()
    pltpu.make_async_copy(
        wsend.at[own_place], wrecv.at[own_place], w_recv.at[own_chunk]
    ).start()

    for c in range(CHUNKS):
        place[c] = jnp.where(slot - c * SLOTS == iota((ROWS, SLOTS), 1), 1.0, 0.0).astype(BF)

    y_copies = {}

    def y_copy(c, i, src, dst, t):
        copy = remote(
            src, dst, y_send.at[c * Y_COPIES + i], y_recv.at[c * Y_COPIES + i], tp_dev(t)
        )
        copy.start()
        y_copies[c, i] = copy

    def gather_first(c, h):
        wait_bytes(recv.at[h, pl.ds(c * PART, PART)], disp_recv.at[2 * c + h])

        def read(b):
            return recv[h, c * PART + b * BLOCK : c * PART + (b + 1) * BLOCK, :]

        def store(b, k, value):
            xg[c, h, 0, b * 16 : (b + 1) * 16, k * 128 : (k + 1) * 128] = value

        from_slots(read, store, perm)
        if h == 0:
            wait_bytes(wrecv.at[pl.ds(c * 16, 16)], w_recv.at[c])
            wgat[c, 0] = jnp.sum(wrecv[c * 16 : (c + 1) * 16].reshape(2, 8, 128), axis=1)
            y_copy(c, 4, wgat.at[c, 0], wgat.at[c, 1], right)
            y_copy(c, 5, wgat.at[c, 0], wgat.at[c, 2], left)
        y_copy(c, 2 * h, xg.at[c, h, 0], xg.at[c, h, 1], right)
        y_copy(c, 2 * h + 1, xg.at[c, h, 0], xg.at[c, h, 2], left)

    def gather_second(c, h):
        if h == 0:
            y_copies[c, 0].wait_recv()
            y_copies[c, 4].wait_recv()
            y_copy(c, 8, wgat.at[c, 1], wgat.at[c, 3], right)
            y_copy(c, 6, xg.at[c, 0, 1], xg.at[c, 0, 3], right)
        else:
            y_copies[c, 3].wait_recv()
            y_copy(c, 7, xg.at[c, 1, 2], xg.at[c, 1, 3], left)

    def experts(c):
        for i in (1, 2, 5, 6, 7, 8):
            y_copies[c, i].wait_recv()
        first = xg[c, 0].reshape(4 * SLOTS, HALF)
        second = xg[c, 1].reshape(4 * SLOTS, HALF)
        gate = dot(first, wg[:HALF, :]) + dot(second, wg[HALF:, :])
        up = dot(first, wu[:HALF, :]) + dot(second, wu[HALF:, :])
        hidden[...] = (gate / (1.0 + jnp.exp(-gate)) * up).astype(BF)
        i, j = iota((4 * SLOTS, 8), 0), iota((4 * SLOTS, 8), 1)
        spread = jnp.where((i * 2731) >> 16 == j, 1.0, 0.0).astype(BF)
        weights = dot(spread, wgat[c].reshape(8, 128).astype(BF))
        i, j = iota((4 * SLOTS, 128), 0), iota((4 * SLOTS, 128), 1)
        i = i - ((i * 2731) >> 16) * 24
        source = (i * 21846) >> 16
        lane = source * 16 + (i - source * CAP) * 4 + tp
        column = jnp.sum(jnp.where(j == lane, weights, 0.0), axis=1, keepdims=True)

        def down(h):
            @pl.loop(0, HALF // 512, unroll=2)
            def _(n):
                at = pl.ds(pl.multiple_of(n * 512, 512), 512)
                wide = pl.ds(pl.multiple_of(n * 512 + h * HALF, 512), 512)
                y = dot(hidden[...], wd[:, wide]).astype(BF).astype(F32)
                part[c, h, :, :, at] = (y * column).astype(BF).reshape(4, SLOTS, 512)

        down(0)
        y_copy(c, 9, part.at[c, 0, 3], ra.at[c], right)
        down(1)
        y_copy(c, 10, part.at[c, 1, 3], rb.at[c], left)
        y_copy(c, 11, part.at[c, 0, 1], fr.at[c, 0], left)

    def add_to(c, h, r, ref):
        @pl.loop(0, HALF // 512, unroll=2)
        def _(n):
            at = pl.ds(pl.multiple_of(n * 512, 512), 512)
            part[c, h, r, :, at] = (
                part[c, h, r, :, at].astype(F32) + ref[c, :, at].astype(F32)
            ).astype(BF)

    def reduce_second(c, h):
        y_copies[c, 9 + h].wait_recv()
        if h == 0:
            add_to(c, 0, 2, ra)
            y_copy(c, 12, part.at[c, 0, 2], fl.at[c, 0], right)
            y_copy(c, 13, part.at[c, 1, 2], fl.at[c, 1], right)
        else:
            add_to(c, 1, 1, rb)
            y_copy(c, 14, part.at[c, 1, 1], fr.at[c, 1], left)

    def give_back(c, h):
        y_copies[c, 12 + h].wait_recv()
        y_copies[c, 11 + 3 * h].wait_recv()

        @pl.loop(0, HALF // 512, unroll=2)
        def _(n):
            at = pl.ds(pl.multiple_of(n * 512, 512), 512)
            mixed[:, at] = (
                part[c, h, 0, :, at].astype(F32)
                + fl[c, h, :, at].astype(F32)
                + fr[c, h, :, at].astype(F32)
            ).astype(BF)

        def read(b, k):
            return mixed[b * 16 : (b + 1) * 16, k * 128 : (k + 1) * 128]

        def store(at, value):
            back[h, c * PART + at : c * PART + at + 128, :] = value

        to_slots(read, store, perm)

        def go(zi, j, p):
            remote(
                back.at[h, message(p)],
                ret.at[h, message(p)],
                back_send,
                back_recv.at[2 * c + h],
                ep_dev(place_from(zi, j)),
            ).start()

        for_partners(c, go)
        if c == own_chunk:
            pltpu.make_async_copy(
                back.at[h, own_rows], ret.at[h, own_rows], back_recv.at[2 * c + h]
            ).start()

    def finish(c, h):
        wait_bytes(ret.at[h, pl.ds(c * PART, PART)], back_recv.at[2 * c + h])

        def read(b):
            return ret[h, c * PART + b * BLOCK : c * PART + (b + 1) * BLOCK, :]

        def store(b, k, value):
            mixed[b * 16 : (b + 1) * 16, k * 128 : (k + 1) * 128] = value

        from_slots(read, store, perm)

        @pl.loop(0, HALF // 512, unroll=2)
        def _(n):
            at = pl.ds(pl.multiple_of(n * 512, 512), 512)
            wide = pl.ds(pl.multiple_of(n * 512 + h * HALF, 512), 512)
            y = dot(place[c], mixed[:, at])
            if c > 0:
                y = y + total[:, wide]
            if c < CHUNKS - 1:
                total[:, wide] = y
            else:
                out_ref[:, wide] = y.astype(BF)

    def attend(pair_of_heads):
        heads = (2 * pair_of_heads, 2 * pair_of_heads + 1)
        gate_columns = jnp.transpose(
            jnp.concatenate([ga[z, xc], jnp.zeros((4, ROWS), F32)], axis=0)
        )

        def step(kb, carried, masked):
            zs = pl.ds(kb * 2, 2)
            k = kv[0, zs].reshape(KEYS, HEAD)
            v = kv[1, zs].reshape(KEYS, HEAD)
            result = []
            for h, (running, norm, acc) in zip(heads, carried):
                q = q_ref[:, h * HEAD : (h + 1) * HEAD]
                gate_k = jnp.concatenate(
                    [ga[kb * 2 + i // 8, i % 8, h : h + 1, :] for i in range(16)], axis=1
                )
                s = lax.dot_general(q, k, (((1,), (1,)), ((), ())), preferred_element_type=F32)
                s = s * SCALE + (gate_columns[:, h : h + 1] - gate_k)
                if masked:
                    behind = me * ROWS - kb * KEYS
                    allowed = iota((ROWS, KEYS), 1) - iota((ROWS, KEYS), 0) <= behind
                    s = jnp.where(allowed, s, NEGATIVE)
                top = jnp.maximum(running, jnp.max(s, axis=1, keepdims=True))
                w = jnp.exp(s - top)
                if masked:
                    w = jnp.where(allowed, w, 0.0)
                factor = jnp.exp(running - top)
                norm = norm * factor + jnp.sum(w, axis=1, keepdims=True)
                acc = acc * factor + dot(w.astype(BF), v)
                result.append((top, norm, acc))
            return tuple(result)

        start = (
            jnp.full((ROWS, 1), NEGATIVE, F32),
            jnp.zeros((ROWS, 1), F32),
            jnp.zeros((ROWS, HEAD), F32),
        )
        last = me // 16
        carried = lax.fori_loop(0, last, lambda kb, c: step(kb, c, False), (start, start))
        for h, (_, norm, acc) in zip(heads, step(last, carried, True)):
            att_ref[:, h * HEAD : (h + 1) * HEAD] = (acc / norm).astype(BF)

    gather_first(0, 0)
    gather_first(0, 1)
    gather_second(0, 0)
    gather_second(0, 1)
    gather_first(1, 0)
    gather_first(1, 1)
    gather_second(1, 0)
    gather_first(2, 0)
    gather_second(1, 1)
    for copy in late_loads:
        copy.wait()
    experts(0)
    gather_second(2, 0)
    gather_first(2, 1)
    reduce_second(0, 0)
    experts(1)
    gather_first(3, 0)
    kv_along_x()
    gather_second(2, 1)
    reduce_second(1, 0)
    gather_first(3, 1)
    reduce_second(1, 1)
    give_back(0, 0)
    give_back(1, 0)
    reduce_second(0, 1)
    gather_second(3, 1)
    experts(2)
    gather_second(3, 0)
    finish(0, 0)
    kv_across()
    give_back(0, 1)
    give_back(1, 1)
    reduce_second(2, 0)
    wait_bytes(kv.at[0], kv_recv.at[6])
    attend(0)
    reduce_second(2, 1)
    experts(3)
    give_back(2, 0)
    finish(1, 0)
    finish(0, 1)
    give_back(2, 1)
    reduce_second(3, 0)
    finish(1, 1)
    reduce_second(3, 1)
    attend(1)
    give_back(3, 0)
    finish(2, 0)
    give_back(3, 1)
    finish(3, 0)
    finish(2, 1)
    finish(3, 1)

    for copy in y_copies.values():
        copy.wait_send()
    sent = pl.ds(0, (NEP - 1) * MSG)
    wait_bytes(send.at[:, sent], disp_send)
    wait_bytes(back.at[:, sent], back_send)
    wait_bytes(wsend.at[pl.ds(0, NEP - 1)], w_send)
    wait_bytes(staged.at[0], kv_send.at[0])
    wait_bytes(ga.at[0, 0], kv_send.at[1])
    wait_bytes(kv.at[0, pl.ds(0, 7), pl.ds(0, 2)], kv_send.at[2])
    wait_bytes(ga.at[pl.ds(0, 7), pl.ds(0, 2)], kv_send.at[3])
    wait_bytes(kv.at[0, :, pl.ds(0, 6)], kv_send.at[4])
    wait_bytes(ga.at[:, pl.ds(0, 6)], kv_send.at[5])
    wait_bytes(kv.at[0], kv_send.at[6])


def per_device(
    queries,
    keys,
    values,
    cum_gates,
    expert_in,
    norm_gain,
    route_group,
    route_member,
    route_weight,
    w_gate,
    w_up,
    w_down,
):
    vmem = pl.BlockSpec(memory_space=pltpu.VMEM)
    hbm = pl.BlockSpec(memory_space=pl.ANY)
    sem = pltpu.SemaphoreType.DMA
    scratch = [
        pltpu.VMEM((ROWS, HEADS * HEAD), BF),
        pltpu.VMEM((1, D), F32),
        pltpu.VMEM((1, ROWS), jnp.int32),
        pltpu.VMEM((2, ROWS), jnp.int32),
        pltpu.VMEM((2, ROWS), F32),
        pltpu.VMEM((ROWS, D), BF),
        pltpu.VMEM((ROWS, D), BF),
        pltpu.VMEM((CHUNKS * SLOTS, D), BF),
        pltpu.VMEM((CHUNKS * SLOTS, ROWS), BF),
        pltpu.VMEM((CHUNKS, ROWS, SLOTS), BF),
        pltpu.VMEM((BLOCK, BLOCK), BF),
        pltpu.VMEM((2, NEP * MSG, 128), BF),
        pltpu.VMEM((2, NEP * MSG, 128), BF),
        pltpu.VMEM((NEP, 1, 128), F32),
        pltpu.VMEM((NEP, 1, 128), F32),
        pltpu.VMEM((CHUNKS, 2, 4, SLOTS, HALF), BF),
        pltpu.VMEM((CHUNKS, 4, 2, 128), F32),
        pltpu.VMEM((CHUNKS, 2, 4, SLOTS, HALF), BF),
        pltpu.VMEM((CHUNKS, SLOTS, HALF), BF),
        pltpu.VMEM((CHUNKS, SLOTS, HALF), BF),
        pltpu.VMEM((CHUNKS, 2, SLOTS, HALF), BF),
        pltpu.VMEM((CHUNKS, 2, SLOTS, HALF), BF),
        pltpu.VMEM((SLOTS, HALF), BF),
        pltpu.VMEM((2, NEP * MSG, 128), BF),
        pltpu.VMEM((2, NEP * MSG, 128), BF),
        pltpu.VMEM((ROWS, D), F32),
        pltpu.VMEM((4 * SLOTS, FF), BF),
        pltpu.VMEM((D, FF), BF),
        pltpu.VMEM((D, FF), BF),
        pltpu.VMEM((FF, D), BF),
        pltpu.VMEM((2, ROWS, HEAD), BF),
        pltpu.VMEM((2, NZ, NX * NC, ROWS, HEAD), BF),
        pltpu.VMEM((NZ, NX * NC, HEADS, ROWS), F32),
        sem((16,)),
        sem,
        sem((2 * CHUNKS,)),
        sem,
        sem((CHUNKS,)),
        sem,
        sem((2 * CHUNKS,)),
        sem((7,)),
        sem((7,)),
        sem((CHUNKS * Y_COPIES,)),
        sem((CHUNKS * Y_COPIES,)),
    ]
    return pl.pallas_call(
        kernel,
        name="step",
        out_shape=(
            pltpu.VMEM((ROWS, HEADS * HEAD), BF),
            pltpu.VMEM((ROWS, D), BF),
        ),
        in_specs=[hbm] * 12,
        out_specs=(vmem, vmem),
        scratch_shapes=scratch,
        compiler_params=pltpu.CompilerParams(
            collective_id=0, has_side_effects=True, vmem_limit_bytes=60 * 1024 * 1024
        ),
    )(
        queries,
        keys,
        values,
        cum_gates.T,
        expert_in,
        norm_gain.reshape(1, D),
        route_group.T,
        route_member.T,
        route_weight.T,
        w_gate[0],
        w_up[0],
        w_down[0],
    )


def solution(mesh):
    return jax.shard_map(
        per_device,
        mesh=mesh,
        in_specs=(
            P("ep", "tp"),
            P("ep", "tp"),
            P("ep", "tp"),
            P("ep", "tp"),
            P(("ep", "tp"), None),
            P(),
            P(("ep", "tp"), None),
            P(("ep", "tp"), None),
            P(("ep", "tp"), None),
            P(("ep", "tp"), None, None),
            P(("ep", "tp"), None, None),
            P(("ep", "tp"), None, None),
        ),
        out_specs=(P("ep", "tp"), P(("ep", "tp"), None)),
        check_vma=False,
    )
```
